32 devices in a mesh: sp: 8 (over z, x), tp: 4 (over y, core).
Axes of the slice: x: 2, y: 2, z: 4, core: 2. Of those that a mesh axis runs over, the one named last changes fastest.
Arguments:
- queries_one: bfloat16 [1024, 2048], P('sp', 'tp'), may hold values from -6.2 to 6.2
- keys_one: bfloat16 [1024, 2048], P('sp', 'tp'), may hold values from -5 to 5
- values_one: bfloat16 [1024, 2048], P('sp', 'tp'), may hold values from -6 to 6
- queries_two: bfloat16 [1024, 1024], P('sp', 'tp'), may hold values from -6.2 to 6.2
- keys_two: bfloat16 [1024, 1024], P('sp', 'tp'), may hold values from -5 to 5
- values_two: bfloat16 [1024, 1024], P('sp', 'tp'), may hold values from -6 to 6
- key_offset: bfloat16 [1024, 2, 16], P('sp', None, 'tp'), may hold values from -14 to 0
- out_one: bfloat16 [2048, 4096], P('tp'), may hold values from -0.109375 to 0.109375
- out_two: bfloat16 [1024, 4096], P('tp'), may hold values from -0.109375 to 0.109375
- residual: bfloat16 [1024, 4096], P('sp', 'tp'), may hold values from -6 to 6
- norm_gain: float32 [4096], replicated, may hold values from 0.1 to 1.9
- routes: int32 [1024, 2], P('sp'), may hold values from 0 to 7, all different within a row; in each aligned block of 128 rows (0 to 127, 128 to 255, ...) at most 64 rows name the same one
- route_weight: float32 [1024, 2], P('sp'), may hold values from 0.2 to 1
- expert_gate: bfloat16 [8, 4096, 2048], P('sp', None, 'tp'), may hold values from -0.09375 to 0.09375
- expert_up: bfloat16 [8, 4096, 2048], P('sp', None, 'tp'), may hold values from -0.09375 to 0.09375
- expert_down: bfloat16 [8, 2048, 4096], P('sp', None, 'tp'), may hold values from -0.125 to 0.125
Outputs:
- mixed: bfloat16 [1024, 4096], P('sp', 'tp')
The draws below stay inside these ranges and needn't reach their ends.
Inputs may be any that keep to these rules, and one draw needn't show every extreme that they name: `routes`: each row names two different experts; in each aligned block of 128 rows no expert is named more than 64 times, a bound that some block reaches.
All inputs are finite; a program needn't handle non-finite values.
Results may differ from the reference program's by a relative error of at most 0.015.
Values may be sent and summed in bfloat16 or wider, within the bound.
A program may use at most 64 MiB of HBM per device.

```python
import math
import jax
import jax.numpy as jnp
import numpy as np
from jax import lax

D = 4096
HEADS = 16
DH1 = 128
DH2 = 64
FFE = 2048
TOK_DEV = 128
TOKENS = 1024
EXPERTS = 8
CAP = 64
N_SP = 8
N_TP = 4


def head_plan(key):
    slow_share = 0.5
    return jax.random.bernoulli(jax.random.fold_in(key, 17), slow_share, (2, HEADS))


def row_plan(key):
    planted_end = max(1, 3 * TOKENS // 32)
    planted = jnp.arange(TOKENS) < planted_end
    aligned = jax.random.bernoulli(jax.random.fold_in(key, 19), 0.25, (TOKENS,))
    return (planted & aligned, planted & jnp.logical_not(aligned))


def direction(key, group, head_size):
    signs = jax.random.bernoulli(jax.random.fold_in(key, 23 + group), 0.5, (HEADS, head_size))
    return signs.astype(jnp.float32) * 2.0 - 1.0


def noise(key, shape):
    return jnp.clip(jax.random.normal(key, shape, jnp.float32), -5.0, 5.0)


def query_draw(key, group, head_size, salt):
    slow = head_plan(key)[group]
    signs = direction(key, group, head_size)
    strength = min(7.0 / head_size ** 0.5, 1.2)
    base = noise(jax.random.fold_in(key, salt), (TOKENS, HEADS, head_size))
    lifted = base + jnp.where(slow[None, :, None], strength * signs[None], 0.0)
    return lifted.reshape(TOKENS, HEADS * head_size).astype(jnp.bfloat16)


def key_draw(key, group, head_size, salt):
    slow = head_plan(key)[group][None, :, None]
    signs = direction(key, group, head_size)
    aligned, decoy = row_plan(key)
    shape = (TOKENS, HEADS, head_size)
    base = noise(jax.random.fold_in(key, salt), shape)
    sizes = jax.random.uniform(jax.random.fold_in(key, salt + 1), shape, jnp.float32, 0.8, 1.2)
    flips = jax.random.bernoulli(jax.random.fold_in(key, salt + 2), 0.5, shape).astype(jnp.float32) * 2.0 - 1.0
    decoy_rows = 3.0 * sizes * flips
    aligned_rows = signs[None] * sizes
    picked = jnp.where(slow & decoy[:, None, None], decoy_rows, base)
    picked = jnp.where(slow & aligned[:, None, None], aligned_rows, picked)
    return picked.reshape(TOKENS, HEADS * head_size).astype(jnp.bfloat16)


def draw_queries_one(key, part):
    return query_draw(key, 0, DH1, 41)


def draw_queries_two(key, part):
    return query_draw(key, 1, DH2, 51)


def draw_keys_one(key, part):
    return key_draw(key, 0, DH1, 61)


def draw_keys_two(key, part):
    return key_draw(key, 1, DH2, 71)


def draw_key_offset(key, part):
    key_blocks, key_rough, key_low, key_high = jax.random.split(jax.random.fold_in(key, 29), 4)
    slow_heads = head_plan(key)
    aligned, decoy = row_plan(key)
    base_rate = jnp.where(slow_heads, -jnp.log(2.0 * TOKENS), -jnp.log(30.0))
    by_block = jax.random.uniform(key_blocks, (TOKENS // TOK_DEV, 2, HEADS), jnp.float32, -0.7, 0.7)
    by_block = jnp.repeat(by_block, TOK_DEV, axis=0)
    roughness = jax.random.uniform(key_rough, (TOKENS, 2, HEADS), jnp.float32, -0.5, 0.5)
    offsets = base_rate[None].astype(jnp.float32) + by_block + roughness
    decoy_level = jax.random.uniform(key_low, (TOKENS, 2, HEADS), jnp.float32, -12.5, -11.5)
    aligned_level = jax.random.uniform(key_high, (TOKENS, 2, HEADS), jnp.float32, -4.5, -3.5)
    slow = slow_heads[None]
    offsets = jnp.where(slow & decoy[:, None, None], decoy_level, offsets)
    offsets = jnp.where(slow & aligned[:, None, None], aligned_level, offsets)
    return offsets.astype(jnp.bfloat16)


def steps_of(own_key, shape, cuts, least, high):
    def one(dim, blocks):
        steps = jax.random.uniform(jax.random.fold_in(jax.random.fold_in(own_key, 6), dim), (blocks,), jnp.float32, least / len(cuts), high / len(cuts))
        return jnp.repeat(jnp.exp(steps), shape[dim] // blocks).reshape((-1,) + (1,) * (len(shape) - dim - 1))

    factor_of = one(*cuts[0])
    for cut in cuts[1:]:
        factor_of = factor_of * one(*cut)
    return factor_of


def shared_out(rng, own, number, rows, amount, top, reach, slope):
    sequence = jax.random.permutation(rng, amount)
    heavy_load, ordinary = shares(amount, rows * top, reach, slope, True), shares(amount, rows * top, reach, slope, False)
    places = jnp.arange(amount)

    def named(lengths, turn):
        used = int((lengths > 0).sum())
        fixed = max(1, used // 4)
        moved = fixed + (places - fixed + turn * (used - fixed)) % max(1, amount - fixed)
        return jnp.zeros((amount,), jnp.int32).at[sequence[jnp.where(places < fixed, places, moved)]].set(jnp.asarray(lengths, jnp.int32))

    lengths = jnp.where(number % 4 == 0, named(heavy_load, number // 4), named(ordinary, number - number // 4 - 1))
    mixed = jax.random.permutation(jax.random.fold_in(own, 3), amount)
    source_of, sink = mixed[0:amount // 2 * 2:2], mixed[1:amount // 2 * 2:2]
    room = jnp.minimum(lengths[source_of] - 1, reach - lengths[sink]) // 2
    room = jnp.where((source_of == sequence[0]) | (sink == sequence[0]) | (lengths[sink] == 0), 0, jnp.maximum(room, 0))
    moved = jax.random.randint(jax.random.fold_in(own, 4), (amount // 2,), 0, 1 << 20) % (room + 1)
    lengths = lengths.at[source_of].add(-moved).at[sink].add(moved)
    members = jnp.searchsorted(jnp.cumsum(lengths), jnp.arange(rows * top), side="right").astype(jnp.int32)
    listing = members.reshape(top, rows).T
    listing = listing[jax.random.permutation(jax.random.fold_in(own, 1), rows)]
    turn = jax.random.randint(jax.random.fold_in(own, 2), (rows, 1), 0, top)
    return jnp.take_along_axis(listing, (jnp.arange(top)[None, :] + turn) % top, axis=1)


def shares(count, total, bound, slope, full):
    portions = [(1 << 20) // math.isqrt(grade ** slope) + 1 for grade in range(1, count + 1)]
    largest = bound if full else min(bound, max(-(-total // count), total * portions[0] // sum(portions)))
    least = 1 if total - largest >= count - 1 else 0
    holding, rest = [largest] + [least] * (count - 1), total - largest - least * (count - 1)
    while rest > 0:
        candidates = [i for i in range(1, count) if holding[i] < largest] or [i for i in range(1, count) if holding[i] < bound]
        whole, remaining = sum([portions[i] for i in candidates]), rest
        for i in candidates:
            extra = min(bound - holding[i], max(1, remaining * portions[i] // whole), rest)
            holding[i] = holding[i] + extra
            rest = rest - extra
    return np.array(holding)


def centred(key, shape, width, bound, pieces=(), kind=jnp.bfloat16):
    values = jax.random.normal(key, shape, jnp.float32) * width
    if len(pieces) > 0:
        values = steps_of(key, shape, pieces, -0.22, 0.18) * values
    return jnp.clip(values, min=-bound, max=bound).astype(kind)


def setup_inputs(seed: int = 0) -> dict:
    seeds = jax.random.split(jax.random.key(seed), 17)
    queries_one = draw_queries_one(jax.random.fold_in(seeds[16], 71), 0)
    keys_one = draw_keys_one(jax.random.fold_in(seeds[16], 71), 0)
    values_one = centred(seeds[2], (TOKENS, HEADS * DH1), 1.0, 6.0, ((0, 8), (1, 4)))
    queries_two = draw_queries_two(jax.random.fold_in(seeds[16], 71), 0)
    keys_two = draw_keys_two(jax.random.fold_in(seeds[16], 71), 0)
    values_two = centred(seeds[5], (TOKENS, HEADS * DH2), 1.0, 6.0, ((0, 8), (1, 4)))
    key_offset = draw_key_offset(jax.random.fold_in(seeds[16], 71), 0)
    out_one = centred(seeds[7], (HEADS * DH1, D), (HEADS * (DH1 + DH2)) ** -0.5, 0.109375, ((0, 4),))
    out_two = centred(seeds[8], (HEADS * DH2, D), (HEADS * (DH1 + DH2)) ** -0.5, 0.109375, ((0, 4),))
    residual = centred(seeds[9], (TOKENS, D), 1.0, 6.0, ((0, 8), (1, 4)))
    norm_gain = jnp.clip(1.0 + 0.18 * jax.random.normal(seeds[10], (D,), jnp.float32), 0.1, 1.9)
    routes_keys = jax.random.split(jax.random.fold_in(seeds[11], 1), TOKENS // TOK_DEV)
    routes_turns = jax.random.permutation(jax.random.fold_in(seeds[11], 3), TOKENS // TOK_DEV)
    routes = jax.vmap(lambda own, number: shared_out(jax.random.fold_in(seeds[11], 2), own, number, TOK_DEV, EXPERTS, 2, CAP, 2))(routes_keys, routes_turns).reshape((TOKENS, 2))
    route_weight = jnp.clip(0.2 + 0.8 * jax.random.uniform(seeds[12], (TOKENS, 2), jnp.float32) ** steps_of(seeds[12], (TOKENS, 2), ((0, 8),), -0.2, 0.2), 0.2, 1.0)
    expert_gate = centred(seeds[13], (EXPERTS, D, FFE), D ** -0.5, 0.09375, ((0, 8), (2, 4)))
    expert_up = centred(seeds[14], (EXPERTS, D, FFE), D ** -0.5, 0.09375, ((0, 8), (2, 4)))
    expert_down = centred(seeds[15], (EXPERTS, FFE, D), FFE ** -0.5, 0.125, ((0, 8), (2, 4)))
    return {"queries_one": queries_one, "keys_one": keys_one, "values_one": values_one, "queries_two": queries_two, "keys_two": keys_two, "values_two": values_two, "key_offset": key_offset, "out_one": out_one, "out_two": out_two, "residual": residual, "norm_gain": norm_gain, "routes": routes, "route_weight": route_weight, "expert_gate": expert_gate, "expert_up": expert_up, "expert_down": expert_down}


EPS = 1e-06

def stick(query, keys, values, offset, head_size):
    total_len, col_count = query.shape
    head_count = col_count // head_size
    query_heads = query.astype(jnp.float32).reshape(total_len // TOK_DEV, TOK_DEV, head_count, head_size)
    key_heads = keys.astype(jnp.float32).reshape(total_len, head_count, head_size)
    value_heads = values.astype(jnp.float32).reshape(total_len, head_count, head_size)
    bias_rows = offset.astype(jnp.float32).T
    key_pos = jnp.arange(total_len, dtype=jnp.int32)

    def one_block(inputs):
        query_block, block_index = inputs
        scores = jnp.einsum('qhd,khd->hqk', query_block, key_heads) * head_size ** (-0.5) + bias_rows[:, None, :]
        query_pos = block_index * TOK_DEV + jnp.arange(TOK_DEV, dtype=jnp.int32)
        causal = key_pos[None, :] < query_pos[:, None]
        log_beta = jax.nn.log_sigmoid(scores)
        log_rest = jnp.where(causal, jax.nn.log_sigmoid(-scores), 0.0)
        shifted = jnp.pad(log_rest[..., 1:], ((0, 0), (0, 0), (0, 1)))
        carried = lax.cumsum(shifted, axis=2, reverse=True)
        weights = jnp.where(causal, jnp.exp(log_beta + carried), 0.0).astype(jnp.bfloat16)
        weights = lax.optimization_barrier(weights)
        result = jnp.einsum('hqk,khd->qhd', weights.astype(jnp.float32), value_heads)
        return result.reshape(TOK_DEV, col_count).astype(jnp.bfloat16)
    blocks_out = lax.map(one_block, (query_heads, jnp.arange(total_len // TOK_DEV, dtype=jnp.int32)))
    return blocks_out.reshape(total_len, col_count)

def reference(queries_one, keys_one, values_one, queries_two, keys_two, values_two, key_offset, out_one, out_two, residual, norm_gain, routes, route_weight, expert_gate, expert_up, expert_down):
    total_len = residual.shape[0]
    attended_one = stick(queries_one, keys_one, values_one, key_offset[:, 0, :], DH1)
    attended_two = stick(queries_two, keys_two, values_two, key_offset[:, 1, :], DH2)
    per_block = HEADS // N_TP
    heads_one = attended_one.reshape(total_len, N_TP, per_block * DH1)
    heads_two = attended_two.reshape(total_len, N_TP, per_block * DH2)
    proj_one = out_one.reshape(N_TP, per_block * DH1, D)
    proj_two = out_two.reshape(N_TP, per_block * DH2, D)

    def add_partial(tp_index, running):
        partial_value = jnp.dot(lax.dynamic_index_in_dim(heads_one, tp_index, 1, keepdims=False), lax.dynamic_index_in_dim(proj_one, tp_index, 0, keepdims=False), preferred_element_type=jnp.float32)
        partial_value = partial_value + jnp.dot(lax.dynamic_index_in_dim(heads_two, tp_index, 1, keepdims=False), lax.dynamic_index_in_dim(proj_two, tp_index, 0, keepdims=False), preferred_element_type=jnp.float32)
        rounded = lax.optimization_barrier(partial_value.astype(jnp.bfloat16))
        return running + rounded.astype(jnp.float32)
    projected = lax.fori_loop(0, N_TP, add_partial, jnp.zeros((total_len, D), jnp.float32))
    stream = (residual.astype(jnp.float32) + projected).astype(jnp.bfloat16)
    stream_f = stream.astype(jnp.float32)
    normed = (stream_f * lax.rsqrt(lax.optimization_barrier(jnp.mean(stream_f * stream_f, axis=1, keepdims=True)) + EPS) * norm_gain).astype(jnp.bfloat16)
    flat_ids = routes.reshape(-1)
    slot_count = N_SP * CAP

    def one_expert(placed, inputs):
        expert_index, gate_w, up_w, down_w = inputs
        is_routed = flat_ids == expert_index
        picked_rows = jnp.nonzero(is_routed, size=slot_count, fill_value=0)[0]
        is_valid = jnp.arange(slot_count) < jnp.sum(is_routed)
        gathered_rows = normed[picked_rows // 2]
        gate_act = jnp.dot(gathered_rows, gate_w, preferred_element_type=jnp.float32)
        up_act = jnp.dot(gathered_rows, up_w, preferred_element_type=jnp.float32)
        hidden = (jax.nn.silu(gate_act) * up_act).astype(jnp.bfloat16)
        expert_result = jnp.dot(hidden, down_w, preferred_element_type=jnp.float32).astype(jnp.bfloat16)
        expert_result = lax.optimization_barrier(expert_result)
        placed = placed.at[picked_rows].add(jnp.where(is_valid[:, None], expert_result.astype(jnp.float32), 0.0))
        return (placed, None)
    placed, _ = lax.scan(one_expert, jnp.zeros((2 * total_len, D), jnp.float32), (jnp.arange(EXPERTS, dtype=jnp.int32), expert_gate, expert_up, expert_down))
    placed = placed.reshape(total_len, 2, D)
    combined = route_weight[:, 0:1] * placed[:, 0] + route_weight[:, 1:2] * placed[:, 1]
    return (stream_f + combined).astype(jnp.bfloat16)
```

```python
import functools

import jax
import jax.numpy as jnp
from jax import lax
from jax.experimental import pallas as pl
from jax.experimental.pallas import tpu as pltpu
from jax.sharding import PartitionSpec as P

DH1 = 128
DH2 = 64


EPS = 1e-06


def stick_group(query, keys, values, offset, head_size, own_start, key_block):
    row_count = query.shape[0]
    head_count = query.shape[1] // head_size
    query_heads = query.reshape(row_count, head_count, head_size)
    query_pos = own_start + jnp.arange(row_count, dtype=jnp.int32)
    block_count = (own_start + row_count + key_block - 1) // key_block

    def key_step(step_index, state_pair):
        summed, carried = state_pair
        first_key = (block_count - 1 - step_index) * key_block
        key_rows = lax.dynamic_slice_in_dim(keys, first_key, key_block, 0).reshape(
            key_block, head_count, head_size
        )
        value_rows = lax.dynamic_slice_in_dim(values, first_key, key_block, 0).reshape(
            key_block, head_count, head_size
        )
        bias_rows = lax.dynamic_slice_in_dim(offset, first_key, key_block, 0).astype(jnp.float32)
        scores = jnp.einsum(
            "qhd,khd->hqk", query_heads, key_rows, preferred_element_type=jnp.float32
        )
        scores = scores * head_size ** (-0.5) + bias_rows.T[:, None, :]
        key_pos = first_key + jnp.arange(key_block, dtype=jnp.int32)
        causal = key_pos[None, :] < query_pos[:, None]
        log_beta = jax.nn.log_sigmoid(scores)
        log_rest = jnp.where(causal, jax.nn.log_sigmoid(-scores), 0.0)
        shifted = jnp.pad(log_rest[..., 1:], ((0, 0), (0, 0), (0, 1)))
        within = lax.cumsum(shifted, axis=2, reverse=True)
        weights = jnp.where(causal, jnp.exp(log_beta + within + carried[..., None]), 0.0).astype(
            jnp.bfloat16
        )
        summed = summed + jnp.einsum(
            "hqk,khd->hqd", weights, value_rows, preferred_element_type=jnp.float32
        )
        carried = carried + jnp.sum(log_rest, axis=2)
        return (summed, carried)

    start_state = (
        jnp.zeros((head_count, row_count, head_size), jnp.float32),
        jnp.zeros((head_count, row_count), jnp.float32),
    )
    summed, _ = lax.fori_loop(0, block_count, key_step, start_state)
    return summed.transpose(1, 0, 2).reshape(row_count, head_count * head_size).astype(jnp.bfloat16)


def body(
    queries_one,
    keys_one,
    values_one,
    queries_two,
    keys_two,
    values_two,
    key_offset,
    out_one,
    out_two,
    residual,
    norm_gain,
    routes,
    route_weight,
    expert_gate,
    expert_up,
    expert_down,
):
    row_count = queries_one.shape[0]
    spread = lax.axis_size("sp")
    tp_count = lax.axis_size("tp")
    own_start = lax.axis_index("sp") * row_count
    factor = max(1, min(spread, 512 // row_count))
    while spread % factor:
        factor -= 1
    key_block = row_count * factor
    far_k1, far_v1, far_k2, far_v2, far_offset = (
        lax.all_gather(keys_one, "sp", axis=0, tiled=True),
        lax.all_gather(values_one, "sp", axis=0, tiled=True),
        lax.all_gather(keys_two, "sp", axis=0, tiled=True),
        lax.all_gather(values_two, "sp", axis=0, tiled=True),
        lax.all_gather(key_offset, "sp", axis=0, tiled=True),
    )
    attended_one = stick_group(
        queries_one, far_k1, far_v1, far_offset[:, 0, :], DH1, own_start, key_block
    )
    attended_two = stick_group(
        queries_two, far_k2, far_v2, far_offset[:, 1, :], DH2, own_start, key_block
    )
    partial_value = jnp.dot(attended_one, out_one, preferred_element_type=jnp.float32)
    partial_value = partial_value + jnp.dot(
        attended_two, out_two, preferred_element_type=jnp.float32
    )
    columns = residual.shape[1]
    column_start = lax.axis_index("tp") * columns
    resid_full = lax.all_gather(residual, "tp", axis=1, tiled=True)
    projected = lax.psum(partial_value.astype(jnp.bfloat16), "tp").astype(jnp.float32)
    stream = (resid_full.astype(jnp.float32) + projected).astype(jnp.bfloat16)
    stream_f = stream.astype(jnp.float32)
    normed = (
        stream_f * lax.rsqrt(jnp.mean(stream_f * stream_f, axis=1, keepdims=True) + EPS) * norm_gain
    ).astype(jnp.bfloat16)
    stream_own = lax.dynamic_slice_in_dim(stream, column_start, columns, 1)
    capacity = tp_count * ((4 * row_count // spread + tp_count - 1) // tp_count)
    flat_ids = routes.reshape(-1)
    onehot = (flat_ids[:, None] == jnp.arange(spread, dtype=jnp.int32)[None, :]).astype(jnp.int32)
    before = jnp.cumsum(onehot, axis=0) - onehot
    slot_of = flat_ids * capacity + jnp.sum(before * onehot, axis=1)
    chosen = slot_of[:, None] == jnp.arange(spread * capacity, dtype=jnp.int32)[None, :]
    selector = jnp.any(chosen.reshape(row_count, 2, spread * capacity), axis=1).T.astype(
        jnp.bfloat16
    )
    outgoing = jnp.dot(selector, normed, preferred_element_type=jnp.float32).astype(jnp.bfloat16)
    outgoing = outgoing.reshape(spread, capacity, normed.shape[1])
    gate_w = expert_gate[0]
    up_w = expert_up[0]
    down_w = expert_down[0]
    share_size = capacity // tp_count
    own_part = lax.dynamic_slice_in_dim(outgoing, lax.axis_index("tp") * share_size, share_size, 1)
    arrived = lax.all_to_all(own_part, "sp", split_axis=0, concat_axis=0, tiled=True)
    arrived = lax.all_gather(arrived, "tp", axis=1, tiled=True)
    sources, items, _ = arrived.shape
    flat_rows = arrived.reshape(sources * items, arrived.shape[2])
    gate_act = jnp.dot(flat_rows, gate_w, preferred_element_type=jnp.float32)
    up_act = jnp.dot(flat_rows, up_w, preferred_element_type=jnp.float32)
    hidden = (jax.nn.silu(gate_act) * up_act).astype(jnp.bfloat16)
    summed = jnp.dot(
        lax.all_gather(hidden, "tp", axis=1, tiled=True), down_w, preferred_element_type=jnp.float32
    )
    returned = lax.all_to_all(
        summed.astype(jnp.bfloat16).reshape(sources, items, down_w.shape[1]),
        "sp",
        split_axis=0,
        concat_axis=0,
        tiled=True,
    )
    back_rows = returned.reshape(spread * capacity, returned.shape[2])
    picked = jnp.dot(chosen.astype(jnp.bfloat16), back_rows, preferred_element_type=jnp.float32)
    picked = picked.reshape(row_count, 2, back_rows.shape[1])
    combined = route_weight[:, 0:1] * picked[:, 0] + route_weight[:, 1:2] * picked[:, 1]
    return (stream_own.astype(jnp.float32) + combined).astype(jnp.bfloat16)


BF = jnp.bfloat16
F32 = jnp.float32


def to(sp, tp):
    return {"device_id": (sp, tp), "device_id_type": pl.DeviceIdType.MESH}


def is_wide(index):
    return (index // 2 + index) % 2 == 0


def flipped(index, mask, n):
    place, total = 1, 0
    while place < n:
        bit = index // place % 2
        total = total + place * (1 - bit if mask & place else bit)
        place *= 2
    return total


def folded(block):
    half = block.shape[0] // 2
    return jnp.concatenate([block[:half, :DH2], block[half:, :DH2]], axis=1)


def unfolded(block):
    return jnp.concatenate([block[:, :DH2], block[:, DH2:]], axis=0)


def turns(n):
    near = list(range(n // 2))
    far = list(range(n - n // 4, n)) + list(range(n // 2, n - n // 4))
    listed, rest = near[:2], near[2:]
    for mask in far:
        listed.append(mask)
        if rest:
            listed.append(rest.pop(0))
    return listed + rest


def neighbours(tp, t):
    partner = tp + 1 - 2 * (tp % 2)
    across = (tp + 2) % t
    return partner, across, across + 1 - 2 * (across % 2)


def layer_kernel(
    n, t, h1, h2, cap,
    off_in, routes, route_weight,
    q1_hbm, k1_hbm, v1_hbm, q2_hbm, k2_hbm, v2_hbm, w1_hbm, w2_hbm, resid_hbm,
    gate_hbm, up_hbm, down_hbm, gain_hbm,
    out,
    q1_in, k1_in, v1_in, q2_in, k2_in, v2_in, w1_in, w2_in, resid_in, gate_in, up_in, down_in, gain,
    pk, pv, buf, off, offbuf, carry, acc, obuf, att,
    pair_out, pair_in, far_out, far_in, stat_out, stat_in, stream_keep, chosen, weights,
    sbuf, xbuf, hbuf, rbuf, backbuf,
    wsem, qs, qr, fs, fr, os_, or_, ps, pr, ys, yr, ss, sr,
    ds_, dr, xs, xr, hs, hr, rs, rr,
):
    in_hbm = (
        q1_hbm, k1_hbm, v1_hbm, q2_hbm, k2_hbm, v2_hbm, w1_hbm, w2_hbm, resid_hbm,
        gate_hbm, up_hbm, down_hbm,
    )
    in_vmem = (
        q1_in, k1_in, v1_in, q2_in, k2_in, v2_in, w1_in, w2_in, resid_in,
        gate_in, up_in, down_in,
    )
    me = lax.axis_index("sp")
    tp = lax.axis_index("tp")
    partner, across, diagonal = neighbours(tp, t)
    rows, cols = resid_in.shape
    peers = [(lax.rem(me + d, n), tp) for d in range(1, n)]
    peers += [(me, peer) for peer in (partner, across, diagonal)]
    barrier = pltpu.get_barrier_semaphore()
    for peer in peers:
        pl.semaphore_signal(barrier, inc=1, **to(*peer))
    own_gain = gain_hbm.at[:, pl.ds(pl.multiple_of(tp * cols, 128), cols)]
    pairs = list(zip(in_hbm, in_vmem)) + [(own_gain, gain)]
    loads = [pltpu.make_async_copy(a, b, wsem.at[i]) for i, (a, b) in enumerate(pairs)]
    for load in loads:
        load.start()
    q1, k1, v1, q2, k2, v2, w1, w2, resid_, gate, up, down = in_vmem
    for load in loads[:6]:
        load.wait()
    for g in range(2):
        for h in range(off_in.shape[1]):
            off[2 * h + (h + g) % 2] = jnp.broadcast_to(off_in[g, h : h + 1, :].astype(F32), (8, rows))
    for h in range(h2):
        lanes = slice(h * DH2, (h + 1) * DH2)
        pk[h] = jnp.concatenate([q2[:, lanes], k2[:, lanes]], axis=1)
        pv[h] = folded(v2[:, lanes])
    pl.semaphore_wait(barrier, len(peers))

    def wide(dest, origin, d, part):
        src = (q1, k1, v1)[part]
        return pltpu.make_async_remote_copy(
            src.at[:, pl.ds(pl.multiple_of(dest // 2 * DH1, DH1), DH1)],
            buf.at[part, origin], qs.at[d, part], qr.at[d, part], **to(dest, tp),
        )

    def narrow(dest, origin, d, part):
        if part:
            src, dst = pv.at[dest // 2], buf.at[2, origin, 0 : rows // 2]
        else:
            src, dst = pk.at[dest // 2], buf.at[0, origin]
        return pltpu.make_async_remote_copy(src, dst, qs.at[d, part], qr.at[d, part], **to(dest, tp))

    def offs(dest, d):
        return pltpu.make_async_remote_copy(
            off.at[dest], offbuf.at[me], fs.at[d], fr.at[d], **to(dest, tp)
        )

    order = [d for pair in zip(range(n // 2, n), range(n // 2)) for d in pair if d]
    for d in order:
        dest = flipped(me, d, n)

        @pl.when(is_wide(dest))
        def _():
            for part in (0, 1, 2):
                wide(dest, me, d, part).start()

        @pl.when(jnp.logical_not(is_wide(dest)))
        def _():
            for part in (0, 2):
                narrow(dest, me, d, part).start()

        offs(dest, d).start()
    offbuf[me] = off[me]

    @pl.when(is_wide(me))
    def _():
        lanes = pl.ds(pl.multiple_of(me // 2 * DH1, DH1), DH1)
        buf[0, me] = q1[:, lanes]
        buf[1, me] = k1[:, lanes]
        buf[2, me] = v1[:, lanes]

    @pl.when(jnp.logical_not(is_wide(me)))
    def _():
        mine = me // 2
        buf[0, me] = pk[mine]
        buf[2, me, 0 : rows // 2] = pv[mine]

    table = jnp.concatenate(
        [routes[...].astype(F32), route_weight[...], jnp.zeros((128 - 4, rows), F32)], axis=0
    ).T
    lane = lax.broadcasted_iota(jnp.int32, (rows, 128), 1)
    row = lax.broadcasted_iota(jnp.int32, (rows, 128), 0)
    named = [table[:, k : k + 1] == lane.astype(F32) for k in (0, 1)]
    either = jnp.where(named[0] | named[1], 1.0, 0.0).astype(BF)
    earlier = jnp.where(lane < row, 1.0, 0.0).astype(BF)
    before = jnp.dot(earlier, either, preferred_element_type=F32)
    slots = lax.broadcasted_iota(jnp.int32, (rows, n * cap), 1).astype(F32)
    for k in (0, 1):
        slot = table[:, k : k + 1] * cap + jnp.sum(
            jnp.where(named[k], before, 0.0), axis=1, keepdims=True
        )
        chosen[k] = jnp.where(slots == slot, 1.0, 0.0).astype(BF)
        weights[k] = jnp.broadcast_to(table[:, 2 + k : 3 + k], (rows, 128))

    lane = lax.broadcasted_iota(jnp.int32, (DH1, 2 * DH1), 1)
    row = lax.broadcasted_iota(jnp.int32, (DH1, 2 * DH1), 0)
    tri = jnp.where((row > lane) | (lane >= DH1), 1.0, 0.0).astype(BF)
    scale = jnp.where(is_wide(me), DH1 ** -0.5, DH2 ** -0.5).astype(F32)
    nt = (((1,), (1,)), ((), ()))

    def blocks(pairs):
        r = lax.broadcasted_iota(jnp.int32, (rows, rows), 0)
        c = lax.broadcasted_iota(jnp.int32, (rows, rows), 1)
        scores = [
            lax.dot_general(buf[0, i], buf[1, j], nt, preferred_element_type=F32)
            for i, j, _ in pairs
        ]
        betas, highs, lows = [], [], []
        for (_, j, own), s in zip(pairs, scores):
            s = s * scale + offbuf[j][0:1, :]
            soft = jnp.log(1.0 + jnp.exp(-jnp.abs(s)))
            log_beta = jnp.minimum(s, 0.0) - soft
            log_rest = log_beta - s
            if own:
                log_rest = jnp.where(c < r, log_rest, 0.0)
            high = log_rest.astype(BF)
            betas.append(log_beta)
            highs.append(high)
            lows.append((log_rest - high.astype(F32)).astype(BF))
        sums = [
            jnp.dot(high, tri, preferred_element_type=F32)
            + jnp.dot(low, tri, preferred_element_type=F32)
            for high, low in zip(highs, lows)
        ]
        weighted = []
        for (i, j, own), log_beta, total in zip(pairs, betas, sums):
            weight = jnp.exp(log_beta + total[:, :DH1])
            if own:
                weight = jnp.where(c < r, weight, 0.0)
            weighted.append(weight.astype(BF))
            carry[i, j] = total[:, DH1:]
        for (i, j, _), weight in zip(pairs, weighted):
            acc[i, j] = jnp.dot(weight, buf[2, j], preferred_element_type=F32)

    here = []
    for d in [0] + order:
        source = flipped(me, d, n)

        @pl.when(is_wide(me))
        def _():
            if d:
                for part in (0, 1, 2):
                    wide(source, me, d, part).wait_recv()

        @pl.when(jnp.logical_not(is_wide(me)))
        def _():
            if d:
                for part in (0, 2):
                    narrow(source, me, d, part).wait_recv()
            both = buf[0, source]
            zero = jnp.zeros((rows, DH1 - DH2), BF)
            buf[1, source] = jnp.concatenate([both[:, DH2:], zero], axis=1)
            buf[0, source] = jnp.concatenate([both[:, :DH2], zero], axis=1)
            buf[2, source] = jnp.concatenate(
                [unfolded(buf[2, source, 0 : rows // 2]), zero], axis=1
            )

        if d:
            offs(source, d).wait_recv()
        blocks(
            [(source, source, True)]
            + [(jnp.maximum(source, k), jnp.minimum(source, k), False) for k in here]
        )
        here.append(source)
    for i in range(n):
        total = acc[i, i]
        passed = carry[i, i]
        for j in range(i - 1, -1, -1):
            total = total + jnp.exp(passed) * acc[i, j]
            passed = passed + carry[i, j]
        obuf[i] = total.astype(BF)

    @pl.when(jnp.logical_not(is_wide(me)))
    def _():
        for i in range(n):
            obuf[i, 0 : rows // 2] = folded(obuf[i])

    def back(dest, d, full):
        part = slice(0, rows if full else rows // 2)
        return pltpu.make_async_remote_copy(
            obuf.at[dest, part], att.at[me, part], os_.at[d], or_.at[d], **to(dest, tp)
        )

    def each(test, act):
        for full in (True, False):

            @pl.when(test if full else jnp.logical_not(test))
            def _():
                act(full)

    each(
        is_wide(me),
        lambda full: [back(flipped(me, d, n), d, full).start() for d in order] and None,
    )
    att[me] = obuf[me]
    for d in order:
        dest = flipped(me, d, n)

        @pl.when(is_wide(dest))
        def _():
            for part in (0, 1, 2):
                wide(dest, me, d, part).wait_send()

        @pl.when(jnp.logical_not(is_wide(dest)))
        def _():
            for part in (0, 2):
                narrow(dest, me, d, part).wait_send()

        offs(dest, d).wait_send()
    for load in loads[6:9] + loads[12:]:
        load.wait()
    for d in order:
        dest = flipped(me, d, n)
        each(is_wide(dest), lambda full: back(dest, d, full).wait_recv())

    a1 = jnp.concatenate([att[2 * h + h % 2] for h in range(h1)], axis=1)
    a2 = jnp.concatenate(
        [unfolded(att[2 * h + 1 - h % 2, 0 : rows // 2]) for h in range(h2)], axis=1
    )

    def partial(target):
        lanes = pl.ds(pl.multiple_of(target * cols, 128), cols)
        return jnp.dot(a1, w1[:, lanes], preferred_element_type=F32) + jnp.dot(
            a2, w2[:, lanes], preferred_element_type=F32
        )

    def pair(slot):
        return pltpu.make_async_remote_copy(
            pair_out.at[slot], pair_in.at[slot], ps.at[slot], pr.at[slot], **to(me, partner)
        )

    far = pltpu.make_async_remote_copy(far_out, far_in, ys.at[0], yr.at[0], **to(me, across))
    pair_out[0] = partial(diagonal).astype(BF)
    pair(0).start()
    there = partial(across)
    pair(0).wait_recv()
    far_out[...] = (there + pair_in[0].astype(F32)).astype(BF)
    far.start()
    each(
        is_wide(me),
        lambda full: [back(flipped(me, d, n), d, full).wait_send() for d in order] and None,
    )
    pair_out[1] = partial(partner).astype(BF)
    pair(1).start()
    here = partial(tp)
    pair(1).wait_recv()
    here = here + pair_in[1].astype(F32)
    far.wait_recv()
    stream = (resid_[...].astype(F32) + (here + far_in[...].astype(F32))).astype(BF)
    stream_keep[...] = stream
    stream = stream.astype(F32)
    squares = jnp.sum(stream * stream, axis=1, keepdims=True)
    stat_out[0] = jnp.broadcast_to(squares, (rows, 128)).T[0:8, :]

    def stat(slot, peer):
        return pltpu.make_async_remote_copy(
            stat_out.at[0], stat_in.at[slot], ss.at[slot], sr.at[slot], **to(me, peer)
        )

    for slot, peer in enumerate((partner, across, diagonal)):
        stat(slot, peer).start()
    for slot, peer in enumerate((partner, across, diagonal)):
        stat(slot, peer).wait_recv()
    total = stat_out[0] + stat_in[0] + stat_in[1] + stat_in[2]
    total = jnp.broadcast_to(total[0:1, :], (128, rows)).T[:, 0:1]
    normed = (stream * lax.rsqrt(total / (t * cols) + EPS) * gain[...]).astype(BF)

    outgoing = lax.dot_general(
        chosen[0] + chosen[1], normed, (((0,), (0,)), ((), ())), preferred_element_type=F32
    ).astype(BF)
    for s in range(n):
        sbuf[s] = outgoing[s * cap : (s + 1) * cap]

    def send(d):
        dest = flipped(me, d, n)
        return pltpu.make_async_remote_copy(
            sbuf.at[dest], xbuf.at[tp, me], ds_.at[d], dr.at[d], **to(dest, tp)
        )

    def spread(ref, sends, recvs, kind, d):
        s = flipped(me, d, n)
        share = across if kind == 2 else tp
        peer = across if kind == 1 else partner
        return pltpu.make_async_remote_copy(
            ref.at[share, s], ref.at[share, s], sends.at[kind, d], recvs.at[kind, d],
            **to(me, peer),
        )

    x_move = functools.partial(spread, xbuf, xs, xr)
    h_move = functools.partial(spread, hbuf, hs, hr)

    def give(d):
        dest = flipped(me, d, n)
        return pltpu.make_async_remote_copy(
            rbuf.at[dest], backbuf.at[me], rs.at[d], rr.at[d], **to(dest, tp)
        )

    listed = turns(n)
    for d in listed[1:]:
        send(d).start()
    xbuf[tp, me] = sbuf[me]
    x_move(1, 0).start()
    x_move(0, 0).start()
    for load in loads[9:12]:
        load.wait()

    def forward(d):
        send(d).wait_recv()
        x_move(1, d).start()
        x_move(0, d).start()

    def relay(move, d):
        move(1, d).wait_recv()
        move(2, d).start()

    def settle(move, d):
        move(0, d).wait_recv()
        move(2, d).wait_recv()

    groups = n // 2

    for g in range(groups + 2):
        if g < groups:
            for d in listed[2 * g : 2 * g + 2]:
                if d:
                    forward(d)
        now = listed[2 * g - 2 : 2 * g] if 1 <= g <= groups else []
        last = listed[2 * g - 4 : 2 * g - 2] if g >= 2 else []
        for d in now:
            relay(x_move, d)
        for d in last:
            relay(h_move, d)
        if now:
            for d in now:
                settle(x_move, d)
            sources = [flipped(me, d, n) for d in now]
            width = xbuf.shape[3]
            gated = jnp.zeros((2 * cap, gate.shape[1]), F32)
            upped = gated
            for j in range(t):
                x = jnp.concatenate([xbuf[j, s] for s in sources], axis=0)
                part = slice(j * width, (j + 1) * width)
                gated = gated + jnp.dot(x, gate[part, :], preferred_element_type=F32)
                upped = upped + jnp.dot(x, up[part, :], preferred_element_type=F32)
            hidden = (gated / (1.0 + jnp.exp(-gated)) * upped).astype(BF)
            for k in (0, 1):
                hbuf[tp, sources[k]] = hidden[k * cap : (k + 1) * cap]
                h_move(1, now[k]).start()
                h_move(0, now[k]).start()
        if last:
            for d in last:
                settle(h_move, d)
            sources = [flipped(me, d, n) for d in last]
            width = hbuf.shape[3]
            done = jnp.zeros((2 * cap, down.shape[1]), F32)
            for j in range(t):
                h = jnp.concatenate([hbuf[j, s] for s in sources], axis=0)
                done = done + jnp.dot(
                    h, down[j * width : (j + 1) * width, :], preferred_element_type=F32
                )
            done = done.astype(BF)
            for k in (0, 1):
                rbuf[sources[k]] = done[k * cap : (k + 1) * cap]
                if last[k]:
                    give(last[k]).start()
    backbuf[me] = rbuf[me]
    for d in range(1, n):
        give(d).wait_recv()
    flat = jnp.concatenate([backbuf[s] for s in range(n)], axis=0)
    total = stream_keep[...].astype(F32)
    for k in (0, 1):
        total = total + weights[k][:, 0:1] * jnp.dot(
            chosen[k], flat, preferred_element_type=F32
        )
    out[...] = total.astype(BF)
    for d in range(n):
        for kind in (0, 1, 2):
            x_move(kind, d).wait_send()
            h_move(kind, d).wait_send()
        if d:
            send(d).wait_send()
            give(d).wait_send()

    pair(0).wait_send()
    pair(1).wait_send()
    far.wait_send()
    for slot, peer in enumerate((partner, across, diagonal)):
        stat(slot, peer).wait_send()


def fast_body(
    queries_one, keys_one, values_one, queries_two, keys_two, values_two, key_offset,
    out_one, out_two, residual, norm_gain, routes, route_weight,
    expert_gate, expert_up, expert_down,
):
    n = lax.axis_size("sp")
    t = lax.axis_size("tp")
    rows, cols = residual.shape
    h1 = queries_one.shape[1] // DH1
    h2 = queries_two.shape[1] // DH2
    cap = 4 * rows // n
    vmem = pl.BlockSpec(memory_space=pltpu.VMEM)
    anyw = pl.BlockSpec(memory_space=pl.ANY)
    dma = pltpu.SemaphoreType.DMA
    large = (
        queries_one, keys_one, values_one, queries_two, keys_two, values_two,
        out_one, out_two, residual, expert_gate[0], expert_up[0], expert_down[0],
    )
    hid = expert_gate.shape[2]
    return pl.pallas_call(
        functools.partial(layer_kernel, n, t, h1, h2, cap),
        out_shape=pltpu.VMEM((rows, cols), BF),
        in_specs=[vmem] * 3 + [anyw] * 13,
        out_specs=vmem,
        scratch_shapes=[pltpu.VMEM(a.shape, a.dtype) for a in large]
        + [
            pltpu.VMEM((1, cols), F32),
            pltpu.VMEM((h2, rows, DH1), BF),
            pltpu.VMEM((h2, rows // 2, DH1), BF),
            pltpu.VMEM((3, n, rows, DH1), BF),
            pltpu.VMEM((n, 8, rows), F32),
            pltpu.VMEM((n, 8, rows), F32),
            pltpu.VMEM((n, n, rows, DH1), F32),
            pltpu.VMEM((n, n, rows, DH1), F32),
            pltpu.VMEM((n, rows, DH1), BF),
            pltpu.VMEM((n, rows, DH1), BF),
            pltpu.VMEM((2, rows, cols), BF),
            pltpu.VMEM((2, rows, cols), BF),
            pltpu.VMEM((rows, cols), BF),
            pltpu.VMEM((rows, cols), BF),
            pltpu.VMEM((1, 8, rows), F32),
            pltpu.VMEM((3, 8, rows), F32),
            pltpu.VMEM((rows, cols), BF),
            pltpu.VMEM((2, rows, n * cap), BF),
            pltpu.VMEM((2, rows, 128), F32),
            pltpu.VMEM((n, cap, cols), BF),
            pltpu.VMEM((t, n, cap, cols), BF),
            pltpu.VMEM((t, n, cap, hid), BF),
            pltpu.VMEM((n, cap, cols), BF),
            pltpu.VMEM((n, cap, cols), BF),
            dma((13,)),
            dma((n, 3)), dma((n, 3)),
            dma((n,)), dma((n,)),
            dma((n,)), dma((n,)),
            dma((2,)), dma((2,)),
            dma((1,)), dma((1,)),
            dma((3,)), dma((3,)),
            dma((n,)), dma((n,)),
            dma((3, n)), dma((3, n)),
            dma((3, n)), dma((3, n)),
            dma((n,)), dma((n,)),
        ],
        compiler_params=pltpu.CompilerParams(
            collective_id=0, has_side_effects=True, vmem_limit_bytes=60 * 2**20
        ),
        name="layer",
    )(
        key_offset.transpose(1, 2, 0), routes.T, route_weight.T, *large, norm_gain[None, :]
    )


def choose(*arrays):
    heads = arrays[0].shape[1] // DH1 + arrays[3].shape[1] // DH2
    n, t = lax.axis_size("sp"), lax.axis_size("tp")
    fits = heads == n and t == 4 and arrays[0].shape[0] == DH1 and DH1 == 2 * DH2
    fits = fits and arrays[0].shape[1] // DH1 * 2 == n and n % 4 == 0 and n & (n - 1) == 0
    return fast_body(*arrays) if fits else body(*arrays)


def solution(mesh):
    return jax.shard_map(
        choose,
        mesh=mesh,
        in_specs=(
            P("sp", "tp"),
            P("sp", "tp"),
            P("sp", "tp"),
            P("sp", "tp"),
            P("sp", "tp"),
            P("sp", "tp"),
            P("sp", None, "tp"),
            P("tp", None),
            P("tp", None),
            P("sp", "tp"),
            P(),
            P("sp", None),
            P("sp", None),
            P("sp", None, "tp"),
            P("sp", None, "tp"),
            P("sp", None, "tp"),
        ),
        out_specs=P("sp", "tp"),
        check_vma=False,
    )
```

```python
import functools

import jax
import jax.numpy as jnp
from jax import lax
from jax.experimental import pallas as pl
from jax.experimental.pallas import tpu as pltpu
from jax.sharding import PartitionSpec as P

DH1 = 128
DH2 = 64


EPS = 1e-06
PIECES = 4
PARTS = 2


def stick_group(query, keys, values, offset, head_size, own_start, key_block):
    row_count = query.shape[0]
    head_count = query.shape[1] // head_size
    query_heads = query.reshape(row_count, head_count, head_size)
    query_pos = own_start + jnp.arange(row_count, dtype=jnp.int32)
    block_count = (own_start + row_count + key_block - 1) // key_block

    def key_step(step_index, state_pair):
        summed, carried = state_pair
        first_key = (block_count - 1 - step_index) * key_block
        key_rows = lax.dynamic_slice_in_dim(keys, first_key, key_block, 0).reshape(
            key_block, head_count, head_size
        )
        value_rows = lax.dynamic_slice_in_dim(values, first_key, key_block, 0).reshape(
            key_block, head_count, head_size
        )
        bias_rows = lax.dynamic_slice_in_dim(offset, first_key, key_block, 0).astype(jnp.float32)
        scores = jnp.einsum(
            "qhd,khd->hqk", query_heads, key_rows, preferred_element_type=jnp.float32
        )
        scores = scores * head_size ** (-0.5) + bias_rows.T[:, None, :]
        key_pos = first_key + jnp.arange(key_block, dtype=jnp.int32)
        causal = key_pos[None, :] < query_pos[:, None]
        log_beta = jax.nn.log_sigmoid(scores)
        log_rest = jnp.where(causal, jax.nn.log_sigmoid(-scores), 0.0)
        shifted = jnp.pad(log_rest[..., 1:], ((0, 0), (0, 0), (0, 1)))
        within = lax.cumsum(shifted, axis=2, reverse=True)
        weights = jnp.where(causal, jnp.exp(log_beta + within + carried[..., None]), 0.0).astype(
            jnp.bfloat16
        )
        summed = summed + jnp.einsum(
            "hqk,khd->hqd", weights, value_rows, preferred_element_type=jnp.float32
        )
        carried = carried + jnp.sum(log_rest, axis=2)
        return (summed, carried)

    start_state = (
        jnp.zeros((head_count, row_count, head_size), jnp.float32),
        jnp.zeros((head_count, row_count), jnp.float32),
    )
    summed, _ = lax.fori_loop(0, block_count, key_step, start_state)
    return summed.transpose(1, 0, 2).reshape(row_count, head_count * head_size).astype(jnp.bfloat16)


def body(
    queries_one,
    keys_one,
    values_one,
    queries_two,
    keys_two,
    values_two,
    key_offset,
    out_one,
    out_two,
    residual,
    norm_gain,
    routes,
    route_weight,
    expert_gate,
    expert_up,
    expert_down,
):
    row_count = queries_one.shape[0]
    spread = lax.axis_size("sp")
    tp_count = lax.axis_size("tp")
    own_start = lax.axis_index("sp") * row_count
    factor = max(1, min(spread, 512 // row_count))
    while spread % factor:
        factor -= 1
    key_block = row_count * factor
    far_k1, far_v1, far_k2, far_v2, far_offset = (
        lax.all_gather(keys_one, "sp", axis=0, tiled=True),
        lax.all_gather(values_one, "sp", axis=0, tiled=True),
        lax.all_gather(keys_two, "sp", axis=0, tiled=True),
        lax.all_gather(values_two, "sp", axis=0, tiled=True),
        lax.all_gather(key_offset, "sp", axis=0, tiled=True),
    )
    attended_one = stick_group(
        queries_one, far_k1, far_v1, far_offset[:, 0, :], DH1, own_start, key_block
    )
    attended_two = stick_group(
        queries_two, far_k2, far_v2, far_offset[:, 1, :], DH2, own_start, key_block
    )
    partial_value = jnp.dot(attended_one, out_one, preferred_element_type=jnp.float32)
    partial_value = partial_value + jnp.dot(
        attended_two, out_two, preferred_element_type=jnp.float32
    )
    columns = residual.shape[1]
    column_start = lax.axis_index("tp") * columns
    resid_full = lax.all_gather(residual, "tp", axis=1, tiled=True)
    projected = lax.psum(partial_value.astype(jnp.bfloat16), "tp").astype(jnp.float32)
    stream = (resid_full.astype(jnp.float32) + projected).astype(jnp.bfloat16)
    stream_f = stream.astype(jnp.float32)
    normed = (
        stream_f * lax.rsqrt(jnp.mean(stream_f * stream_f, axis=1, keepdims=True) + EPS) * norm_gain
    ).astype(jnp.bfloat16)
    stream_own = lax.dynamic_slice_in_dim(stream, column_start, columns, 1)
    capacity = tp_count * ((4 * row_count // spread + tp_count - 1) // tp_count)
    flat_ids = routes.reshape(-1)
    onehot = (flat_ids[:, None] == jnp.arange(spread, dtype=jnp.int32)[None, :]).astype(jnp.int32)
    before = jnp.cumsum(onehot, axis=0) - onehot
    slot_of = flat_ids * capacity + jnp.sum(before * onehot, axis=1)
    chosen = slot_of[:, None] == jnp.arange(spread * capacity, dtype=jnp.int32)[None, :]
    selector = jnp.any(chosen.reshape(row_count, 2, spread * capacity), axis=1).T.astype(
        jnp.bfloat16
    )
    outgoing = jnp.dot(selector, normed, preferred_element_type=jnp.float32).astype(jnp.bfloat16)
    outgoing = outgoing.reshape(spread, capacity, normed.shape[1])
    gate_w = expert_gate[0]
    up_w = expert_up[0]
    down_w = expert_down[0]
    share_size = capacity // tp_count
    own_part = lax.dynamic_slice_in_dim(outgoing, lax.axis_index("tp") * share_size, share_size, 1)
    arrived = lax.all_to_all(own_part, "sp", split_axis=0, concat_axis=0, tiled=True)
    arrived = lax.all_gather(arrived, "tp", axis=1, tiled=True)
    sources, items, _ = arrived.shape
    flat_rows = arrived.reshape(sources * items, arrived.shape[2])
    gate_act = jnp.dot(flat_rows, gate_w, preferred_element_type=jnp.float32)
    up_act = jnp.dot(flat_rows, up_w, preferred_element_type=jnp.float32)
    hidden = (jax.nn.silu(gate_act) * up_act).astype(jnp.bfloat16)
    summed = jnp.dot(
        lax.all_gather(hidden, "tp", axis=1, tiled=True), down_w, preferred_element_type=jnp.float32
    )
    returned = lax.all_to_all(
        summed.astype(jnp.bfloat16).reshape(sources, items, down_w.shape[1]),
        "sp",
        split_axis=0,
        concat_axis=0,
        tiled=True,
    )
    back_rows = returned.reshape(spread * capacity, returned.shape[2])
    picked = jnp.dot(chosen.astype(jnp.bfloat16), back_rows, preferred_element_type=jnp.float32)
    picked = picked.reshape(row_count, 2, back_rows.shape[1])
    combined = route_weight[:, 0:1] * picked[:, 0] + route_weight[:, 1:2] * picked[:, 1]
    return (stream_own.astype(jnp.float32) + combined).astype(jnp.bfloat16)


BF = jnp.bfloat16
F32 = jnp.float32


def to(sp, tp):
    return {"device_id": (sp, tp), "device_id_type": pl.DeviceIdType.MESH}


def is_wide(index):
    return (index // 2 + index) % 2 == 0


def flipped(index, mask, n):
    place, total = 1, 0
    while place < n:
        bit = index // place % 2
        total = total + place * (1 - bit if mask & place else bit)
        place *= 2
    return total


def folded(block):
    half = block.shape[0] // 2
    return jnp.concatenate([block[:half, :DH2], block[half:, :DH2]], axis=1)


def unfolded(block):
    return jnp.concatenate([block[:, :DH2], block[:, DH2:]], axis=0)


SENDS = (
    ((1, 0), (4, 0), (2, 0)),
    ((4, 1), (1, 1), (2, 1)),
    ((5, 0), (5, 1), (3, 0), (3, 1), (6, 0), (6, 1), (7, 0), (7, 1)),
)
STEPS = (
    ("f", 1), ("f", 2), ("s"), ("f", 4), ("r", 0), ("r", 1), ("f", 5), ("r", 2), ("f", 3), ("r", 4),
    ("x", 4, 1), ("r", 5), ("f", 6), ("x", 5, 2), ("r", 3), ("h", 4, 1), ("f", 7), ("r", 6),
    ("x", 6, 3), ("h", 5, 2), ("r", 7), ("x", 7, 0), ("h", 6, 3), ("h", 7, 0),
)


def neighbours(tp, t):
    partner = tp + 1 - 2 * (tp % 2)
    across = (tp + 2) % t
    return partner, across, across + 1 - 2 * (across % 2)


def layer_kernel(
    n, t, h1, h2, cap,
    off_in, routes, route_weight,
    q1_hbm, k1_hbm, v1_hbm, q2_hbm, k2_hbm, v2_hbm, w1_hbm, w2_hbm, resid_hbm,
    gate_hbm, up_hbm, down_hbm, gain_hbm,
    out,
    q1_in, k1_in, v1_in, q2_in, k2_in, v2_in, w_in, resid_in, gate_in, up_in, down_in, gain,
    pk, pv, buf, off, offbuf, carry, acc, obuf, att,
    pair_out, pair_in, far_out, far_in, mine, stat_out, stat_in, fac_out, fac_in,
    stream_keep, scaled, chosen, picker, weights,
    sbuf, xbuf, hbuf, rbuf, backbuf,
    wsem, qs, qr, fs, fr, os_, or_, ps, pr, ys, yr, ss, sr, cs, cr,
    ds_, dr, xs, xr, hs, hr, rs, rr,
):
    in_hbm = (
        q1_hbm, k1_hbm, v1_hbm, q2_hbm, k2_hbm, v2_hbm, w1_hbm, w2_hbm, resid_hbm,
        gate_hbm, up_hbm, down_hbm,
    )
    in_vmem = (
        q1_in, k1_in, v1_in, q2_in, k2_in, v2_in,
        w_in.at[0 : h1 * DH1], w_in.at[h1 * DH1 :], resid_in, gate_in, up_in, down_in,
    )
    me = lax.axis_index("sp")
    tp = lax.axis_index("tp")
    partner, across, diagonal = neighbours(tp, t)
    rows, cols = resid_in.shape
    peers = [(lax.rem(me + d, n), tp) for d in range(1, n)]
    peers += [(me, peer) for peer in (partner, across, diagonal)]
    barrier = pltpu.get_barrier_semaphore()
    for peer in peers:
        pl.semaphore_signal(barrier, inc=1, **to(*peer))
    own_gain = gain_hbm.at[:, pl.ds(pl.multiple_of(tp * cols, 128), cols)]
    pairs = list(zip(in_hbm, in_vmem)) + [(own_gain, gain)]
    loads = [pltpu.make_async_copy(a, b, wsem.at[i]) for i, (a, b) in enumerate(pairs)]
    for load in loads:
        load.start()
    q1, k1, v1, q2, k2, v2 = in_vmem[:6]
    gate, up, down = in_vmem[9:]
    for load in loads[:6]:
        load.wait()
    for g in range(2):
        for h in range(off_in.shape[1]):
            off[2 * h + (h + g) % 2] = jnp.broadcast_to(off_in[g, h : h + 1, :].astype(F32), (8, rows))
    for h in range(h2):
        lanes = slice(h * DH2, (h + 1) * DH2)
        pk[h] = jnp.concatenate([q2[:, lanes], k2[:, lanes]], axis=1)
        pv[h] = folded(v2[:, lanes])
    pl.semaphore_wait(barrier, len(peers))

    def wide(dest, origin, d, part):
        src = (q1, k1, v1)[part]
        return pltpu.make_async_remote_copy(
            src.at[:, pl.ds(pl.multiple_of(dest // 2 * DH1, DH1), DH1)],
            buf.at[part, origin], qs.at[d, part], qr.at[d, part], **to(dest, tp),
        )

    def narrow(dest, origin, d, part):
        if part:
            src, dst = pv.at[dest // 2], buf.at[2, origin, 0 : rows // 2]
        else:
            src, dst = pk.at[dest // 2], buf.at[0, origin]
        return pltpu.make_async_remote_copy(src, dst, qs.at[d, part], qr.at[d, part], **to(dest, tp))

    def offs(dest, d):
        return pltpu.make_async_remote_copy(
            off.at[dest], offbuf.at[me], fs.at[d], fr.at[d], **to(dest, tp)
        )

    order = [d for pair in zip(range(n // 2, n), range(n // 2)) for d in pair if d]
    for d in order:
        dest = flipped(me, d, n)

        @pl.when(is_wide(dest))
        def _():
            for part in (0, 1, 2):
                wide(dest, me, d, part).start()

        @pl.when(jnp.logical_not(is_wide(dest)))
        def _():
            for part in (0, 2):
                narrow(dest, me, d, part).start()

        offs(dest, d).start()
    offbuf[me] = off[me]

    @pl.when(is_wide(me))
    def _():
        lanes = pl.ds(pl.multiple_of(me // 2 * DH1, DH1), DH1)
        buf[0, me] = q1[:, lanes]
        buf[1, me] = k1[:, lanes]
        buf[2, me] = v1[:, lanes]

    @pl.when(jnp.logical_not(is_wide(me)))
    def _():
        mine = me // 2
        buf[0, me] = pk[mine]
        buf[2, me, 0 : rows // 2] = pv[mine]

    table = jnp.concatenate(
        [routes[...].astype(F32), route_weight[...], jnp.zeros((128 - 4, rows), F32)], axis=0
    ).T
    lane = lax.broadcasted_iota(jnp.int32, (rows, 128), 1)
    row = lax.broadcasted_iota(jnp.int32, (rows, 128), 0)
    named = [table[:, k : k + 1] == lane.astype(F32) for k in (0, 1)]
    either = jnp.where(named[0] | named[1], 1.0, 0.0).astype(BF)
    earlier = jnp.where(lane < row, 1.0, 0.0).astype(BF)
    before = jnp.dot(earlier, either, preferred_element_type=F32)
    slots = lax.broadcasted_iota(jnp.int32, (rows, n * cap), 1).astype(F32)
    for k in (0, 1):
        slot = table[:, k : k + 1] * cap + jnp.sum(
            jnp.where(named[k], before, 0.0), axis=1, keepdims=True
        )
        chosen[k] = jnp.where(slots == slot, 1.0, 0.0).astype(BF)
        weights[k] = jnp.broadcast_to(table[:, 2 + k : 3 + k], (rows, 128))
    picker[...] = (chosen[0] + chosen[1]).astype(F32).T.astype(BF)

    lane = lax.broadcasted_iota(jnp.int32, (DH1, 2 * DH1), 1)
    row = lax.broadcasted_iota(jnp.int32, (DH1, 2 * DH1), 0)
    tri = jnp.where((row > lane) | (lane >= DH1), 1.0, 0.0).astype(BF)
    scale = jnp.where(is_wide(me), DH1 ** -0.5, DH2 ** -0.5).astype(F32)
    nt = (((1,), (1,)), ((), ()))

    def blocks(pairs):
        r = lax.broadcasted_iota(jnp.int32, (rows, rows), 0)
        c = lax.broadcasted_iota(jnp.int32, (rows, rows), 1)
        scores = [
            lax.dot_general(buf[0, i], buf[1, j], nt, preferred_element_type=F32)
            for i, j, _ in pairs
        ]
        betas, highs, lows = [], [], []
        for (_, j, own), s in zip(pairs, scores):
            s = s * scale + offbuf[j][0:1, :]
            soft = jnp.log(1.0 + jnp.exp(-jnp.abs(s)))
            log_beta = jnp.minimum(s, 0.0) - soft
            log_rest = log_beta - s
            if own:
                log_rest = jnp.where(c < r, log_rest, 0.0)
            high = log_rest.astype(BF)
            betas.append(log_beta)
            highs.append(high)
            lows.append((log_rest - high.astype(F32)).astype(BF))
        sums = [
            jnp.dot(high, tri, preferred_element_type=F32)
            + jnp.dot(low, tri, preferred_element_type=F32)
            for high, low in zip(highs, lows)
        ]
        weighted = []
        for (i, j, own), log_beta, total in zip(pairs, betas, sums):
            weight = jnp.exp(log_beta + total[:, :DH1])
            if own:
                weight = jnp.where(c < r, weight, 0.0)
            weighted.append(weight.astype(BF))
            carry[i, j] = total[:, DH1:]
        for (i, j, _), weight in zip(pairs, weighted):
            acc[i, j] = jnp.dot(weight, buf[2, j], preferred_element_type=F32)

    here = []
    for d in [0] + order:
        source = flipped(me, d, n)

        @pl.when(is_wide(me))
        def _():
            if d:
                for part in (0, 1, 2):
                    wide(source, me, d, part).wait_recv()

        @pl.when(jnp.logical_not(is_wide(me)))
        def _():
            if d:
                for part in (0, 2):
                    narrow(source, me, d, part).wait_recv()
            both = buf[0, source]
            zero = jnp.zeros((rows, DH1 - DH2), BF)
            buf[1, source] = jnp.concatenate([both[:, DH2:], zero], axis=1)
            buf[0, source] = jnp.concatenate([both[:, :DH2], zero], axis=1)
            buf[2, source] = jnp.concatenate(
                [unfolded(buf[2, source, 0 : rows // 2]), zero], axis=1
            )

        if d:
            offs(source, d).wait_recv()
        blocks(
            [(source, source, True)]
            + [(jnp.maximum(source, k), jnp.minimum(source, k), False) for k in here]
        )
        here.append(source)
    for i in range(n):
        total = acc[i, i]
        passed = carry[i, i]
        for j in range(i - 1, -1, -1):
            total = total + jnp.exp(passed) * acc[i, j]
            passed = passed + carry[i, j]
        obuf[i] = total.astype(BF)

    @pl.when(jnp.logical_not(is_wide(me)))
    def _():
        for i in range(n):
            obuf[i, 0 : rows // 2] = folded(obuf[i])

    def back(dest, d, full):
        part = slice(0, rows if full else rows // 2)
        return pltpu.make_async_remote_copy(
            obuf.at[dest, part], att.at[me, part], os_.at[d], or_.at[d], **to(dest, tp)
        )

    def each(test, act):
        for full in (True, False):

            @pl.when(test if full else jnp.logical_not(test))
            def _():
                act(full)

    each(
        is_wide(me),
        lambda full: [back(flipped(me, d, n), d, full).start() for d in order] and None,
    )
    att[me] = obuf[me]
    for d in order:
        dest = flipped(me, d, n)

        @pl.when(is_wide(dest))
        def _():
            for part in (0, 1, 2):
                wide(dest, me, d, part).wait_send()

        @pl.when(jnp.logical_not(is_wide(dest)))
        def _():
            for part in (0, 2):
                narrow(dest, me, d, part).wait_send()

        offs(dest, d).wait_send()
    for load in loads[6:9] + loads[12:]:
        load.wait()
    for d in order:
        dest = flipped(me, d, n)
        each(is_wide(dest), lambda full: back(dest, d, full).wait_recv())

    a1 = jnp.concatenate([att[2 * h + h % 2] for h in range(h1)], axis=1)
    a2 = jnp.concatenate(
        [unfolded(att[2 * h + 1 - h % 2, 0 : rows // 2]) for h in range(h2)], axis=1
    )

    a = jnp.concatenate([a1, a2], axis=1)
    pieces, _, width = mine.shape

    def partial(target, c):
        lanes = pl.ds(pl.multiple_of(target * cols + c * width, 128), width)
        return jnp.dot(a, w_in[:, lanes], preferred_element_type=F32)

    def pair(slot, c):
        return pltpu.make_async_remote_copy(
            pair_out.at[slot, c], pair_in.at[slot, c], ps.at[slot, c], pr.at[slot, c],
            **to(me, partner),
        )

    def far(c):
        return pltpu.make_async_remote_copy(
            far_out.at[c], far_in.at[c], ys.at[c], yr.at[c], **to(me, across)
        )

    for c in range(pieces):
        pair_out[0, c] = partial(diagonal, c).astype(BF)
        pair(0, c).start()
    for c in range(pieces):
        there = partial(across, c)
        pair(0, c).wait_recv()
        far_out[c] = (there + pair_in[0, c].astype(F32)).astype(BF)
        far(c).start()
    for c in range(pieces):
        pair_out[1, c] = partial(partner, c).astype(BF)
        pair(1, c).start()
    each(
        is_wide(me),
        lambda full: [back(flipped(me, d, n), d, full).wait_send() for d in order] and None,
    )
    for c in range(pieces):
        own = partial(tp, c)
        pair(1, c).wait_recv()
        mine[c] = own + pair_in[1, c].astype(F32)
    parts, _, _, wide_part = sbuf.shape
    per = pieces // parts

    def stat(slot, peer):
        return pltpu.make_async_remote_copy(
            stat_out.at[0], stat_in.at[slot], ss.at[slot], sr.at[slot], **to(me, peer)
        )

    def send(d, p):
        dest = flipped(me, d, n)
        return pltpu.make_async_remote_copy(
            sbuf.at[p, dest], xbuf.at[tp, p, me], ds_.at[d, p], dr.at[d, p], **to(dest, tp)
        )

    def x_move(kind, d, p):
        s = flipped(me, d, n)
        share = across if kind == 2 else tp
        peer = across if kind == 1 else partner
        return pltpu.make_async_remote_copy(
            xbuf.at[share, p, s], xbuf.at[share, p, s], xs.at[kind, d, p], xr.at[kind, d, p],
            **to(me, peer),
        )

    def h_move(kind, d):
        s = flipped(me, d, n)
        share = across if kind == 2 else tp
        peer = across if kind == 1 else partner
        return pltpu.make_async_remote_copy(
            hbuf.at[share, s], hbuf.at[share, s], hs.at[kind, d], hr.at[kind, d],
            **to(me, peer),
        )

    def factor(d):
        dest = flipped(me, d, n)
        return pltpu.make_async_remote_copy(
            fac_out.at[dest], fac_in.at[me], cs.at[d], cr.at[d], **to(dest, tp)
        )

    peers = tuple(enumerate((partner, across, diagonal)))
    squares = jnp.zeros((rows, 1), F32)
    for c in range(pieces):
        lanes = slice(c * width, (c + 1) * width)
        far(c).wait_recv()
        stream = (resid_in[:, lanes].astype(F32) + (mine[c] + far_in[c].astype(F32))).astype(BF)
        stream_keep[:, lanes] = stream
        stream = stream.astype(F32)
        scaled[:, lanes] = (stream * gain[:, lanes]).astype(BF)
        squares = squares + jnp.sum(stream * stream, axis=1, keepdims=True)
        if c == pieces - 1:
            stat_out[0] = jnp.broadcast_to(squares, (rows, 128)).T[0:8, :]
            for slot, peer in peers:
                stat(slot, peer).start()
        if (c + 1) % per == 0:
            p = c // per
            part = slice(p * wide_part, (p + 1) * wide_part)
            outgoing = jnp.dot(
                picker[...], scaled[:, part], preferred_element_type=F32
            ).astype(BF)
            for s in range(n):
                sbuf[p, s] = outgoing[s * cap : (s + 1) * cap]
            for d, q in SENDS[p]:
                send(d, q).start()
            xbuf[tp, p, me] = sbuf[p, me]
            x_move(1, 0, p).start()
            x_move(0, 0, p).start()
    def norms():
        for slot, peer in peers:
            stat(slot, peer).wait_recv()
        total = stat_out[0] + stat_in[0] + stat_in[1] + stat_in[2]
        total = jnp.broadcast_to(total[0:1, :], (128, rows)).T[:, 0:1]
        inverse = lax.rsqrt(total / (t * cols) + EPS)
        inverse = jnp.sum(
            (chosen[0] + chosen[1]).astype(F32) * inverse, axis=0, keepdims=True
        )
        for s in range(n):
            spot = inverse[:, s * cap : (s + 1) * cap]
            spot = jnp.concatenate([spot, jnp.zeros((1, 128 - cap), F32)], axis=1)
            fac_out[s] = jnp.broadcast_to(spot, (8, 128))
        for d in order:
            factor(d).start()
        fac_in[me] = fac_out[me]
        for d, q in SENDS[-1]:
            send(d, q).start()

    def give(d):
        dest = flipped(me, d, n)
        return pltpu.make_async_remote_copy(
            rbuf.at[dest], backbuf.at[me], rs.at[d], rr.at[d], **to(dest, tp)
        )

    for load in loads[9:12]:
        load.wait()

    def relay(move):
        move(1).wait_recv()
        move(2).start()

    def settle(move):
        move(0).wait_recv()
        move(2).wait_recv()

    def enter(members):
        for d in members:
            if d:
                factor(d).wait_recv()
            for p in range(parts):
                settle(lambda kind: x_move(kind, d, p))
        sources = [flipped(me, d, n) for d in members]
        column = jnp.concatenate([fac_in[s][0:1, :cap] for s in sources], axis=1)
        column = jnp.broadcast_to(column, (128, len(members) * cap)).T[:, 0:1]
        gated = jnp.zeros((len(members) * cap, gate.shape[1]), F32)
        upped = gated
        for j in range(t):
            for p in range(parts):
                x = jnp.concatenate([xbuf[j, p, s] for s in sources], axis=0)
                first = j * cols + p * wide_part
                gated = gated + jnp.dot(
                    x, gate[first : first + wide_part, :], preferred_element_type=F32
                )
                upped = upped + jnp.dot(
                    x, up[first : first + wide_part, :], preferred_element_type=F32
                )
        gated = gated * column
        hidden = (gated / (1.0 + jnp.exp(-gated)) * (upped * column)).astype(BF)
        for k, d in enumerate(members):
            hbuf[tp, sources[k]] = hidden[k * cap : (k + 1) * cap]
            h_move(1, d).start()
            h_move(0, d).start()

    def leave(members):
        for d in members:
            relay(lambda kind: h_move(kind, d))
        for d in members:
            settle(lambda kind: h_move(kind, d))
        sources = [flipped(me, d, n) for d in members]
        size = hbuf.shape[3]
        done = jnp.zeros((len(members) * cap, down.shape[1]), F32)
        for j in range(t):
            h = jnp.concatenate([hbuf[j, s] for s in sources], axis=0)
            done = done + jnp.dot(
                h, down[j * size : (j + 1) * size, :], preferred_element_type=F32
            )
        done = done.astype(BF)
        for k, d in enumerate(members):
            rbuf[sources[k]] = done[k * cap : (k + 1) * cap]
            if d:
                give(d).start()

    for kind, *members in STEPS:
        if kind == "s":
            norms()
        elif kind == "f":
            for p in range(parts):
                send(members[0], p).wait_recv()
                x_move(1, members[0], p).start()
                x_move(0, members[0], p).start()
        elif kind == "r":
            for p in range(parts):
                relay(lambda k: x_move(k, members[0], p))
        elif kind == "x":
            enter(members)
        else:
            if (kind, *members) == STEPS[-1]:
                for d in range(n):
                    for p in range(parts):
                        for k in (0, 1, 2):
                            x_move(k, d, p).wait_send()
                        if d:
                            send(d, p).wait_send()
                    if d:
                        factor(d).wait_send()
                for c in range(pieces):
                    pair(0, c).wait_send()
                    pair(1, c).wait_send()
                    far(c).wait_send()
                for slot, peer in peers:
                    stat(slot, peer).wait_send()
            leave(members)
    backbuf[me] = rbuf[me]
    for d in range(1, n):
        give(d).wait_recv()
    flat = jnp.concatenate([backbuf[s] for s in range(n)], axis=0)
    total = stream_keep[...].astype(F32)
    for k in (0, 1):
        total = total + weights[k][:, 0:1] * jnp.dot(
            chosen[k], flat, preferred_element_type=F32
        )
    out[...] = total.astype(BF)
    for d in range(n):
        for kind in (0, 1, 2):
            h_move(kind, d).wait_send()
        if d:
            give(d).wait_send()


def fast_body(
    queries_one, keys_one, values_one, queries_two, keys_two, values_two, key_offset,
    out_one, out_two, residual, norm_gain, routes, route_weight,
    expert_gate, expert_up, expert_down,
):
    n = lax.axis_size("sp")
    t = lax.axis_size("tp")
    rows, cols = residual.shape
    h1 = queries_one.shape[1] // DH1
    h2 = queries_two.shape[1] // DH2
    cap = 4 * rows // n
    vmem = pl.BlockSpec(memory_space=pltpu.VMEM)
    anyw = pl.BlockSpec(memory_space=pl.ANY)
    dma = pltpu.SemaphoreType.DMA
    large = (
        queries_one, keys_one, values_one, queries_two, keys_two, values_two,
        out_one, out_two, residual, expert_gate[0], expert_up[0], expert_down[0],
    )
    hid = expert_gate.shape[2]
    return pl.pallas_call(
        functools.partial(layer_kernel, n, t, h1, h2, cap),
        out_shape=pltpu.VMEM((rows, cols), BF),
        in_specs=[vmem] * 3 + [anyw] * 13,
        out_specs=vmem,
        scratch_shapes=[pltpu.VMEM(a.shape, a.dtype) for a in large[:6]]
        + [pltpu.VMEM((out_one.shape[0] + out_two.shape[0], out_one.shape[1]), BF)]
        + [pltpu.VMEM(a.shape, a.dtype) for a in large[8:]]
        + [
            pltpu.VMEM((1, cols), F32),
            pltpu.VMEM((h2, rows, DH1), BF),
            pltpu.VMEM((h2, rows // 2, DH1), BF),
            pltpu.VMEM((3, n, rows, DH1), BF),
            pltpu.VMEM((n, 8, rows), F32),
            pltpu.VMEM((n, 8, rows), F32),
            pltpu.VMEM((n, n, rows, DH1), F32),
            pltpu.VMEM((n, n, rows, DH1), F32),
            pltpu.VMEM((n, rows, DH1), BF),
            pltpu.VMEM((n, rows, DH1), BF),
            pltpu.VMEM((2, PIECES, rows, cols // PIECES), BF),
            pltpu.VMEM((2, PIECES, rows, cols // PIECES), BF),
            pltpu.VMEM((PIECES, rows, cols // PIECES), BF),
            pltpu.VMEM((PIECES, rows, cols // PIECES), BF),
            pltpu.VMEM((PIECES, rows, cols // PIECES), F32),
            pltpu.VMEM((1, 8, rows), F32),
            pltpu.VMEM((3, 8, rows), F32),
            pltpu.VMEM((n, 8, 128), F32),
            pltpu.VMEM((n, 8, 128), F32),
            pltpu.VMEM((rows, cols), BF),
            pltpu.VMEM((rows, cols), BF),
            pltpu.VMEM((2, rows, n * cap), BF),
            pltpu.VMEM((n * cap, rows), BF),
            pltpu.VMEM((2, rows, 128), F32),
            pltpu.VMEM((PARTS, n, cap, cols // PARTS), BF),
            pltpu.VMEM((t, PARTS, n, cap, cols // PARTS), BF),
            pltpu.VMEM((t, n, cap, hid), BF),
            pltpu.VMEM((n, cap, cols), BF),
            pltpu.VMEM((n, cap, cols), BF),
            dma((13,)),
            dma((n, 3)), dma((n, 3)),
            dma((n,)), dma((n,)),
            dma((n,)), dma((n,)),
            dma((2, PIECES)), dma((2, PIECES)),
            dma((PIECES,)), dma((PIECES,)),
            dma((3,)), dma((3,)),
            dma((n,)), dma((n,)),
            dma((n, PARTS)), dma((n, PARTS)),
            dma((3, n, PARTS)), dma((3, n, PARTS)),
            dma((3, n)), dma((3, n)),
            dma((n,)), dma((n,)),
        ],
        compiler_params=pltpu.CompilerParams(
            collective_id=0, has_side_effects=True, vmem_limit_bytes=60 * 2**20
        ),
        name="layer",
    )(
        key_offset.transpose(1, 2, 0), routes.T, route_weight.T, *large, norm_gain[None, :]
    )


def choose(*arrays):
    heads = arrays[0].shape[1] // DH1 + arrays[3].shape[1] // DH2
    n, t = lax.axis_size("sp"), lax.axis_size("tp")
    fits = heads == n and t == 4 and arrays[0].shape[0] == DH1 and DH1 == 2 * DH2
    fits = fits and arrays[0].shape[1] // DH1 * 2 == n and n == 8 and DH1 * 4 // n * 2 == 128
    return fast_body(*arrays) if fits else body(*arrays)


def solution(mesh):
    return jax.shard_map(
        choose,
        mesh=mesh,
        in_specs=(
            P("sp", "tp"),
            P("sp", "tp"),
            P("sp", "tp"),
            P("sp", "tp"),
            P("sp", "tp"),
            P("sp", "tp"),
            P("sp", None, "tp"),
            P("tp", None),
            P("tp", None),
            P("sp", "tp"),
            P(),
            P("sp", None),
            P("sp", None),
            P("sp", None, "tp"),
            P("sp", None, "tp"),
            P("sp", None, "tp"),
        ),
        out_specs=P("sp", "tp"),
        check_vma=False,
    )
```

```python
import functools

import jax
import jax.numpy as jnp
from jax import lax
from jax.experimental import pallas as pl
from jax.experimental.pallas import tpu as pltpu
from jax.sharding import PartitionSpec as P

DH1 = 128
DH2 = 64


EPS = 1e-06
PIECES = 4
PARTS = 2


def stick_group(query, keys, values, offset, head_size, own_start, key_block):
    row_count = query.shape[0]
    head_count = query.shape[1] // head_size
    query_heads = query.reshape(row_count, head_count, head_size)
    query_pos = own_start + jnp.arange(row_count, dtype=jnp.int32)
    block_count = (own_start + row_count + key_block - 1) // key_block

    def key_step(step_index, state_pair):
        summed, carried = state_pair
        first_key = (block_count - 1 - step_index) * key_block
        key_rows = lax.dynamic_slice_in_dim(keys, first_key, key_block, 0).reshape(
            key_block, head_count, head_size
        )
        value_rows = lax.dynamic_slice_in_dim(values, first_key, key_block, 0).reshape(
            key_block, head_count, head_size
        )
        bias_rows = lax.dynamic_slice_in_dim(offset, first_key, key_block, 0).astype(jnp.float32)
        scores = jnp.einsum(
            "qhd,khd->hqk", query_heads, key_rows, preferred_element_type=jnp.float32
        )
        scores = scores * head_size ** (-0.5) + bias_rows.T[:, None, :]
        key_pos = first_key + jnp.arange(key_block, dtype=jnp.int32)
        causal = key_pos[None, :] < query_pos[:, None]
        log_beta = jax.nn.log_sigmoid(scores)
        log_rest = jnp.where(causal, jax.nn.log_sigmoid(-scores), 0.0)
        shifted = jnp.pad(log_rest[..., 1:], ((0, 0), (0, 0), (0, 1)))
        within = lax.cumsum(shifted, axis=2, reverse=True)
        weights = jnp.where(causal, jnp.exp(log_beta + within + carried[..., None]), 0.0).astype(
            jnp.bfloat16
        )
        summed = summed + jnp.einsum(
            "hqk,khd->hqd", weights, value_rows, preferred_element_type=jnp.float32
        )
        carried = carried + jnp.sum(log_rest, axis=2)
        return (summed, carried)

    start_state = (
        jnp.zeros((head_count, row_count, head_size), jnp.float32),
        jnp.zeros((head_count, row_count), jnp.float32),
    )
    summed, _ = lax.fori_loop(0, block_count, key_step, start_state)
    return summed.transpose(1, 0, 2).reshape(row_count, head_count * head_size).astype(jnp.bfloat16)


def body(
    queries_one,
    keys_one,
    values_one,
    queries_two,
    keys_two,
    values_two,
    key_offset,
    out_one,
    out_two,
    residual,
    norm_gain,
    routes,
    route_weight,
    expert_gate,
    expert_up,
    expert_down,
):
    row_count = queries_one.shape[0]
    spread = lax.axis_size("sp")
    tp_count = lax.axis_size("tp")
    own_start = lax.axis_index("sp") * row_count
    factor = max(1, min(spread, 512 // row_count))
    while spread % factor:
        factor -= 1
    key_block = row_count * factor
    far_k1, far_v1, far_k2, far_v2, far_offset = (
        lax.all_gather(keys_one, "sp", axis=0, tiled=True),
        lax.all_gather(values_one, "sp", axis=0, tiled=True),
        lax.all_gather(keys_two, "sp", axis=0, tiled=True),
        lax.all_gather(values_two, "sp", axis=0, tiled=True),
        lax.all_gather(key_offset, "sp", axis=0, tiled=True),
    )
    attended_one = stick_group(
        queries_one, far_k1, far_v1, far_offset[:, 0, :], DH1, own_start, key_block
    )
    attended_two = stick_group(
        queries_two, far_k2, far_v2, far_offset[:, 1, :], DH2, own_start, key_block
    )
    partial_value = jnp.dot(attended_one, out_one, preferred_element_type=jnp.float32)
    partial_value = partial_value + jnp.dot(
        attended_two, out_two, preferred_element_type=jnp.float32
    )
    columns = residual.shape[1]
    column_start = lax.axis_index("tp") * columns
    resid_full = lax.all_gather(residual, "tp", axis=1, tiled=True)
    projected = lax.psum(partial_value.astype(jnp.bfloat16), "tp").astype(jnp.float32)
    stream = (resid_full.astype(jnp.float32) + projected).astype(jnp.bfloat16)
    stream_f = stream.astype(jnp.float32)
    normed = (
        stream_f * lax.rsqrt(jnp.mean(stream_f * stream_f, axis=1, keepdims=True) + EPS) * norm_gain
    ).astype(jnp.bfloat16)
    stream_own = lax.dynamic_slice_in_dim(stream, column_start, columns, 1)
    capacity = tp_count * ((4 * row_count // spread + tp_count - 1) // tp_count)
    flat_ids = routes.reshape(-1)
    onehot = (flat_ids[:, None] == jnp.arange(spread, dtype=jnp.int32)[None, :]).astype(jnp.int32)
    before = jnp.cumsum(onehot, axis=0) - onehot
    slot_of = flat_ids * capacity + jnp.sum(before * onehot, axis=1)
    chosen = slot_of[:, None] == jnp.arange(spread * capacity, dtype=jnp.int32)[None, :]
    selector = jnp.any(chosen.reshape(row_count, 2, spread * capacity), axis=1).T.astype(
        jnp.bfloat16
    )
    outgoing = jnp.dot(selector, normed, preferred_element_type=jnp.float32).astype(jnp.bfloat16)
    outgoing = outgoing.reshape(spread, capacity, normed.shape[1])
    gate_w = expert_gate[0]
    up_w = expert_up[0]
    down_w = expert_down[0]
    share_size = capacity // tp_count
    own_part = lax.dynamic_slice_in_dim(outgoing, lax.axis_index("tp") * share_size, share_size, 1)
    arrived = lax.all_to_all(own_part, "sp", split_axis=0, concat_axis=0, tiled=True)
    arrived = lax.all_gather(arrived, "tp", axis=1, tiled=True)
    sources, items, _ = arrived.shape
    flat_rows = arrived.reshape(sources * items, arrived.shape[2])
    gate_act = jnp.dot(flat_rows, gate_w, preferred_element_type=jnp.float32)
    up_act = jnp.dot(flat_rows, up_w, preferred_element_type=jnp.float32)
    hidden = (jax.nn.silu(gate_act) * up_act).astype(jnp.bfloat16)
    summed = jnp.dot(
        lax.all_gather(hidden, "tp", axis=1, tiled=True), down_w, preferred_element_type=jnp.float32
    )
    returned = lax.all_to_all(
        summed.astype(jnp.bfloat16).reshape(sources, items, down_w.shape[1]),
        "sp",
        split_axis=0,
        concat_axis=0,
        tiled=True,
    )
    back_rows = returned.reshape(spread * capacity, returned.shape[2])
    picked = jnp.dot(chosen.astype(jnp.bfloat16), back_rows, preferred_element_type=jnp.float32)
    picked = picked.reshape(row_count, 2, back_rows.shape[1])
    combined = route_weight[:, 0:1] * picked[:, 0] + route_weight[:, 1:2] * picked[:, 1]
    return (stream_own.astype(jnp.float32) + combined).astype(jnp.bfloat16)


BF = jnp.bfloat16
F32 = jnp.float32


def to(sp, tp):
    return {"device_id": (sp, tp), "device_id_type": pl.DeviceIdType.MESH}


def is_wide(index):
    return (index // 2 + index) % 2 == 0


def flipped(index, mask, n):
    place, total = 1, 0
    while place < n:
        bit = index // place % 2
        total = total + place * (1 - bit if mask & place else bit)
        place *= 2
    return total


def folded(block):
    half = block.shape[0] // 2
    return jnp.concatenate([block[:half, :DH2], block[half:, :DH2]], axis=1)


def unfolded(block):
    return jnp.concatenate([block[:, :DH2], block[:, DH2:]], axis=0)


SENDS = (
    ((1, 0), (4, 0)),
    ((4, 1), (1, 1), (2, 0), (2, 1), (5, 0)),
    ((5, 1), (3, 0), (3, 1), (6, 0), (6, 1), (7, 0), (7, 1)),
)
STEPS = (
    ("f", 1), ("f", 4), ("s"), ("f", 2), ("r", 0), ("r", 1), ("r", 4), ("f", 5), ("x", 4, 1),
    ("r", 2), ("f", 3), ("r", 5), ("x", 5, 2), ("f", 6), ("q", 4), ("q", 1), ("r", 3), ("h", 4, 1),
    ("f", 7), ("q", 5), ("q", 2), ("h", 5, 2), ("r", 6), ("x", 6, 3), ("r", 7), ("x", 7, 0), ("q", 6),
    ("q", 3), ("h", 6, 3), ("q", 7), ("q", 0), ("h", 7, 0),
)


def neighbours(tp, t):
    partner = tp + 1 - 2 * (tp % 2)
    across = (tp + 2) % t
    return partner, across, across + 1 - 2 * (across % 2)


def layer_kernel(
    n, t, h1, h2, cap,
    off_in, routes, route_weight,
    q1_hbm, k1_hbm, v1_hbm, q2_hbm, k2_hbm, v2_hbm, w1_hbm, w2_hbm, resid_hbm,
    gate_hbm, up_hbm, down_hbm, gain_hbm,
    out,
    q1_in, k1_in, v1_in, q2_in, k2_in, v2_in, w_in, resid_in, gate_in, up_in, down_in, gain,
    pk, pv, buf, off, offbuf, carry, acc, obuf, att,
    pair_out, pair_in, far_out, far_in, mine, stat_out, stat_in, fac_out, fac_in,
    stream_keep, scaled, chosen, picker, weights,
    sbuf, xbuf, hbuf, rbuf, backbuf,
    wsem, qs, qr, fs, fr, os_, or_, ps, pr, ys, yr, ss, sr, cs, cr,
    ds_, dr, xs, xr, hs, hr, rs, rr,
):
    in_hbm = (
        q1_hbm, k1_hbm, v1_hbm, q2_hbm, k2_hbm, v2_hbm, w1_hbm, w2_hbm, resid_hbm,
        gate_hbm, up_hbm, down_hbm,
    )
    in_vmem = (
        q1_in, k1_in, v1_in, q2_in, k2_in, v2_in,
        w_in.at[0 : h1 * DH1], w_in.at[h1 * DH1 :], resid_in, gate_in, up_in, down_in,
    )
    me = lax.axis_index("sp")
    tp = lax.axis_index("tp")
    partner, across, diagonal = neighbours(tp, t)
    rows, cols = resid_in.shape
    peers = [(lax.rem(me + d, n), tp) for d in range(1, n)]
    peers += [(me, peer) for peer in (partner, across, diagonal)]
    barrier = pltpu.get_barrier_semaphore()
    for peer in peers:
        pl.semaphore_signal(barrier, inc=1, **to(*peer))
    own_gain = gain_hbm.at[:, pl.ds(pl.multiple_of(tp * cols, 128), cols)]
    pairs = list(zip(in_hbm, in_vmem)) + [(own_gain, gain)]
    loads = [pltpu.make_async_copy(a, b, wsem.at[i]) for i, (a, b) in enumerate(pairs)]
    for load in loads:
        load.start()
    q1, k1, v1, q2, k2, v2 = in_vmem[:6]
    gate, up, down = in_vmem[9:]
    for load in loads[:6]:
        load.wait()
    for g in range(2):
        for h in range(off_in.shape[1]):
            off[2 * h + (h + g) % 2] = jnp.broadcast_to(off_in[g, h : h + 1, :].astype(F32), (8, rows))
    for h in range(h2):
        lanes = slice(h * DH2, (h + 1) * DH2)
        pk[h] = jnp.concatenate([q2[:, lanes], k2[:, lanes]], axis=1)
        pv[h] = folded(v2[:, lanes])
    pl.semaphore_wait(barrier, len(peers))

    def wide(dest, origin, d, part):
        src = (q1, k1, v1)[part]
        return pltpu.make_async_remote_copy(
            src.at[:, pl.ds(pl.multiple_of(dest // 2 * DH1, DH1), DH1)],
            buf.at[part, origin], qs.at[d, part], qr.at[d, part], **to(dest, tp),
        )

    def narrow(dest, origin, d, part):
        if part:
            src, dst = pv.at[dest // 2], buf.at[2, origin, 0 : rows // 2]
        else:
            src, dst = pk.at[dest // 2], buf.at[0, origin]
        return pltpu.make_async_remote_copy(src, dst, qs.at[d, part], qr.at[d, part], **to(dest, tp))

    def offs(dest, d):
        return pltpu.make_async_remote_copy(
            off.at[dest], offbuf.at[me], fs.at[d], fr.at[d], **to(dest, tp)
        )

    order = [d for pair in zip(range(n // 2, n), range(n // 2)) for d in pair if d]
    for d in order:
        dest = flipped(me, d, n)

        @pl.when(is_wide(dest))
        def _():
            for part in (0, 1, 2):
                wide(dest, me, d, part).start()

        @pl.when(jnp.logical_not(is_wide(dest)))
        def _():
            for part in (0, 2):
                narrow(dest, me, d, part).start()

        offs(dest, d).start()
    offbuf[me] = off[me]

    @pl.when(is_wide(me))
    def _():
        lanes = pl.ds(pl.multiple_of(me // 2 * DH1, DH1), DH1)
        buf[0, me] = q1[:, lanes]
        buf[1, me] = k1[:, lanes]
        buf[2, me] = v1[:, lanes]

    @pl.when(jnp.logical_not(is_wide(me)))
    def _():
        mine = me // 2
        buf[0, me] = pk[mine]
        buf[2, me, 0 : rows // 2] = pv[mine]

    table = jnp.concatenate(
        [routes[...].astype(F32), route_weight[...], jnp.zeros((128 - 4, rows), F32)], axis=0
    ).T
    lane = lax.broadcasted_iota(jnp.int32, (rows, 128), 1)
    row = lax.broadcasted_iota(jnp.int32, (rows, 128), 0)
    named = [table[:, k : k + 1] == lane.astype(F32) for k in (0, 1)]
    either = jnp.where(named[0] | named[1], 1.0, 0.0).astype(BF)
    earlier = jnp.where(lane < row, 1.0, 0.0).astype(BF)
    before = jnp.dot(earlier, either, preferred_element_type=F32)
    slots = lax.broadcasted_iota(jnp.int32, (rows, n * cap), 1).astype(F32)
    for k in (0, 1):
        slot = table[:, k : k + 1] * cap + jnp.sum(
            jnp.where(named[k], before, 0.0), axis=1, keepdims=True
        )
        chosen[k] = jnp.where(slots == slot, 1.0, 0.0).astype(BF)
        weights[k] = jnp.broadcast_to(table[:, 2 + k : 3 + k], (rows, 128))
    picker[...] = (chosen[0] + chosen[1]).astype(F32).T.astype(BF)

    lane = lax.broadcasted_iota(jnp.int32, (DH1, 2 * DH1), 1)
    row = lax.broadcasted_iota(jnp.int32, (DH1, 2 * DH1), 0)
    tri = jnp.where((row > lane) | (lane >= DH1), 1.0, 0.0).astype(BF)
    scale = jnp.where(is_wide(me), DH1 ** -0.5, DH2 ** -0.5).astype(F32)
    nt = (((1,), (1,)), ((), ()))

    def blocks(pairs):
        r = lax.broadcasted_iota(jnp.int32, (rows, rows), 0)
        c = lax.broadcasted_iota(jnp.int32, (rows, rows), 1)
        scores = [
            lax.dot_general(buf[0, i], buf[1, j], nt, preferred_element_type=F32)
            for i, j, _ in pairs
        ]
        betas, highs, lows = [], [], []
        for (_, j, own), s in zip(pairs, scores):
            s = s * scale + offbuf[j][0:1, :]
            soft = jnp.log(1.0 + jnp.exp(-jnp.abs(s)))
            log_beta = jnp.minimum(s, 0.0) - soft
            log_rest = log_beta - s
            if own:
                log_rest = jnp.where(c < r, log_rest, 0.0)
            high = log_rest.astype(BF)
            betas.append(log_beta)
            highs.append(high)
            lows.append((log_rest - high.astype(F32)).astype(BF))
        sums = [
            jnp.dot(high, tri, preferred_element_type=F32)
            + jnp.dot(low, tri, preferred_element_type=F32)
            for high, low in zip(highs, lows)
        ]
        weighted = []
        for (i, j, own), log_beta, total in zip(pairs, betas, sums):
            weight = jnp.exp(log_beta + total[:, :DH1])
            if own:
                weight = jnp.where(c < r, weight, 0.0)
            weighted.append(weight.astype(BF))
            carry[i, j] = total[:, DH1:]
        for (i, j, _), weight in zip(pairs, weighted):
            acc[i, j] = jnp.dot(weight, buf[2, j], preferred_element_type=F32)

    here = []
    for d in [0] + order:
        source = flipped(me, d, n)

        @pl.when(is_wide(me))
        def _():
            if d:
                for part in (0, 1, 2):
                    wide(source, me, d, part).wait_recv()

        @pl.when(jnp.logical_not(is_wide(me)))
        def _():
            if d:
                for part in (0, 2):
                    narrow(source, me, d, part).wait_recv()
            both = buf[0, source]
            zero = jnp.zeros((rows, DH1 - DH2), BF)
            buf[1, source] = jnp.concatenate([both[:, DH2:], zero], axis=1)
            buf[0, source] = jnp.concatenate([both[:, :DH2], zero], axis=1)
            buf[2, source] = jnp.concatenate(
                [unfolded(buf[2, source, 0 : rows // 2]), zero], axis=1
            )

        if d:
            offs(source, d).wait_recv()
        blocks(
            [(source, source, True)]
            + [(jnp.maximum(source, k), jnp.minimum(source, k), False) for k in here]
        )
        here.append(source)
    for i in range(n):
        total = acc[i, i]
        passed = carry[i, i]
        for j in range(i - 1, -1, -1):
            total = total + jnp.exp(passed) * acc[i, j]
            passed = passed + carry[i, j]
        obuf[i] = total.astype(BF)

    @pl.when(jnp.logical_not(is_wide(me)))
    def _():
        for i in range(n):
            obuf[i, 0 : rows // 2] = folded(obuf[i])

    def back(dest, d, full):
        part = slice(0, rows if full else rows // 2)
        return pltpu.make_async_remote_copy(
            obuf.at[dest, part], att.at[me, part], os_.at[d], or_.at[d], **to(dest, tp)
        )

    def each(test, act):
        for full in (True, False):

            @pl.when(test if full else jnp.logical_not(test))
            def _():
                act(full)

    each(
        is_wide(me),
        lambda full: [back(flipped(me, d, n), d, full).start() for d in order] and None,
    )
    att[me] = obuf[me]
    for d in order:
        dest = flipped(me, d, n)

        @pl.when(is_wide(dest))
        def _():
            for part in (0, 1, 2):
                wide(dest, me, d, part).wait_send()

        @pl.when(jnp.logical_not(is_wide(dest)))
        def _():
            for part in (0, 2):
                narrow(dest, me, d, part).wait_send()

        offs(dest, d).wait_send()
    for load in loads[6:9] + loads[12:]:
        load.wait()
    for d in order:
        dest = flipped(me, d, n)
        each(is_wide(dest), lambda full: back(dest, d, full).wait_recv())

    a1 = jnp.concatenate([att[2 * h + h % 2] for h in range(h1)], axis=1)
    a2 = jnp.concatenate(
        [unfolded(att[2 * h + 1 - h % 2, 0 : rows // 2]) for h in range(h2)], axis=1
    )

    a = jnp.concatenate([a1, a2], axis=1)
    pieces, _, width = mine.shape

    def partial(target, c):
        lanes = pl.ds(pl.multiple_of(target * cols + c * width, 128), width)
        return jnp.dot(a, w_in[:, lanes], preferred_element_type=F32)

    def pair(slot, c):
        return pltpu.make_async_remote_copy(
            pair_out.at[slot, c], pair_in.at[slot, c], ps.at[slot, c], pr.at[slot, c],
            **to(me, partner),
        )

    def far(c):
        return pltpu.make_async_remote_copy(
            far_out.at[c], far_in.at[c], ys.at[c], yr.at[c], **to(me, across)
        )

    for c in range(pieces):
        pair_out[0, c] = partial(diagonal, c).astype(BF)
        pair(0, c).start()
    for c in range(pieces):
        there = partial(across, c)
        pair(0, c).wait_recv()
        far_out[c] = (there + pair_in[0, c].astype(F32)).astype(BF)
        far(c).start()
    for c in range(pieces):
        pair_out[1, c] = partial(partner, c).astype(BF)
        pair(1, c).start()
    each(
        is_wide(me),
        lambda full: [back(flipped(me, d, n), d, full).wait_send() for d in order] and None,
    )
    for c in range(pieces):
        own = partial(tp, c)
        pair(1, c).wait_recv()
        mine[c] = own + pair_in[1, c].astype(F32)
    parts, _, _, wide_part = sbuf.shape
    per = pieces // parts

    def stat(slot, peer):
        return pltpu.make_async_remote_copy(
            stat_out.at[0], stat_in.at[slot], ss.at[slot], sr.at[slot], **to(me, peer)
        )

    def send(d, p):
        dest = flipped(me, d, n)
        return pltpu.make_async_remote_copy(
            sbuf.at[p, dest], xbuf.at[tp, p, me], ds_.at[d, p], dr.at[d, p], **to(dest, tp)
        )

    def x_move(kind, d, p):
        s = flipped(me, d, n)
        share = across if kind == 2 else tp
        peer = across if kind == 1 else partner
        return pltpu.make_async_remote_copy(
            xbuf.at[share, p, s], xbuf.at[share, p, s], xs.at[kind, d, p], xr.at[kind, d, p],
            **to(me, peer),
        )

    def h_move(kind, d):
        s = flipped(me, d, n)
        share = across if kind == 2 else tp
        peer = across if kind == 1 else partner
        return pltpu.make_async_remote_copy(
            hbuf.at[share, s], hbuf.at[share, s], hs.at[kind, d], hr.at[kind, d],
            **to(me, peer),
        )

    def factor(d):
        dest = flipped(me, d, n)
        return pltpu.make_async_remote_copy(
            fac_out.at[dest], fac_in.at[me], cs.at[d], cr.at[d], **to(dest, tp)
        )

    peers = tuple(enumerate((partner, across, diagonal)))
    squares = jnp.zeros((rows, 1), F32)
    for c in range(pieces):
        lanes = slice(c * width, (c + 1) * width)
        far(c).wait_recv()
        stream = (resid_in[:, lanes].astype(F32) + (mine[c] + far_in[c].astype(F32))).astype(BF)
        stream_keep[:, lanes] = stream
        stream = stream.astype(F32)
        scaled[:, lanes] = (stream * gain[:, lanes]).astype(BF)
        squares = squares + jnp.sum(stream * stream, axis=1, keepdims=True)
        if c == pieces - 1:
            stat_out[0] = jnp.broadcast_to(squares, (rows, 128)).T[0:8, :]
            for slot, peer in peers:
                stat(slot, peer).start()
        if (c + 1) % per == 0:
            p = c // per
            part = slice(p * wide_part, (p + 1) * wide_part)
            outgoing = jnp.dot(
                picker[...], scaled[:, part], preferred_element_type=F32
            ).astype(BF)
            for s in range(n):
                sbuf[p, s] = outgoing[s * cap : (s + 1) * cap]
            for d, q in SENDS[p]:
                send(d, q).start()
            xbuf[tp, p, me] = sbuf[p, me]
            x_move(1, 0, p).start()
            x_move(0, 0, p).start()
    def norms():
        for slot, peer in peers:
            stat(slot, peer).wait_recv()
        total = stat_out[0] + stat_in[0] + stat_in[1] + stat_in[2]
        total = jnp.broadcast_to(total[0:1, :], (128, rows)).T[:, 0:1]
        inverse = lax.rsqrt(total / (t * cols) + EPS)
        inverse = jnp.sum(
            (chosen[0] + chosen[1]).astype(F32) * inverse, axis=0, keepdims=True
        )
        for s in range(n):
            spot = inverse[:, s * cap : (s + 1) * cap]
            spot = jnp.concatenate([spot, jnp.zeros((1, 128 - cap), F32)], axis=1)
            fac_out[s] = jnp.broadcast_to(spot, (8, 128))
        for d in order:
            factor(d).start()
        fac_in[me] = fac_out[me]
        for d, q in SENDS[-1]:
            send(d, q).start()

    def give(d):
        dest = flipped(me, d, n)
        return pltpu.make_async_remote_copy(
            rbuf.at[dest], backbuf.at[me], rs.at[d], rr.at[d], **to(dest, tp)
        )

    for load in loads[9:12]:
        load.wait()

    def relay(move):
        move(1).wait_recv()
        move(2).start()

    def settle(move):
        move(0).wait_recv()
        move(2).wait_recv()

    def enter(members):
        for d in members:
            if d:
                factor(d).wait_recv()
            for p in range(parts):
                settle(lambda kind: x_move(kind, d, p))
        sources = [flipped(me, d, n) for d in members]
        column = jnp.concatenate([fac_in[s][0:1, :cap] for s in sources], axis=1)
        column = jnp.broadcast_to(column, (128, len(members) * cap)).T[:, 0:1]
        gated = jnp.zeros((len(members) * cap, gate.shape[1]), F32)
        upped = gated
        for j in range(t):
            for p in range(parts):
                x = jnp.concatenate([xbuf[j, p, s] for s in sources], axis=0)
                first = j * cols + p * wide_part
                gated = gated + jnp.dot(
                    x, gate[first : first + wide_part, :], preferred_element_type=F32
                )
                upped = upped + jnp.dot(
                    x, up[first : first + wide_part, :], preferred_element_type=F32
                )
        gated = gated * column
        hidden = (gated / (1.0 + jnp.exp(-gated)) * (upped * column)).astype(BF)
        for k, d in enumerate(members):
            hbuf[tp, sources[k]] = hidden[k * cap : (k + 1) * cap]
            h_move(1, d).start()
            h_move(0, d).start()

    def leave(members):
        for d in members:
            settle(lambda kind: h_move(kind, d))
        sources = [flipped(me, d, n) for d in members]
        size = hbuf.shape[3]
        done = jnp.zeros((len(members) * cap, down.shape[1]), F32)
        for j in range(t):
            h = jnp.concatenate([hbuf[j, s] for s in sources], axis=0)
            done = done + jnp.dot(
                h, down[j * size : (j + 1) * size, :], preferred_element_type=F32
            )
        done = done.astype(BF)
        for k, d in enumerate(members):
            rbuf[sources[k]] = done[k * cap : (k + 1) * cap]
            if d:
                give(d).start()

    for kind, *members in STEPS:
        if kind == "s":
            norms()
        elif kind == "f":
            for p in range(parts):
                send(members[0], p).wait_recv()
                x_move(1, members[0], p).start()
                x_move(0, members[0], p).start()
        elif kind == "r":
            for p in range(parts):
                relay(lambda k: x_move(k, members[0], p))
        elif kind == "x":
            enter(members)
        elif kind == "q":
            relay(lambda k: h_move(k, members[0]))
        else:
            if (kind, *members) == STEPS[-1]:
                for d in range(n):
                    for p in range(parts):
                        for k in (0, 1, 2):
                            x_move(k, d, p).wait_send()
                        if d:
                            send(d, p).wait_send()
                    if d:
                        factor(d).wait_send()
                for c in range(pieces):
                    pair(0, c).wait_send()
                    pair(1, c).wait_send()
                    far(c).wait_send()
                for slot, peer in peers:
                    stat(slot, peer).wait_send()
            leave(members)
    backbuf[me] = rbuf[me]
    for d in range(1, n):
        give(d).wait_recv()
    flat = jnp.concatenate([backbuf[s] for s in range(n)], axis=0)
    total = stream_keep[...].astype(F32)
    for k in (0, 1):
        total = total + weights[k][:, 0:1] * jnp.dot(
            chosen[k], flat, preferred_element_type=F32
        )
    out[...] = total.astype(BF)
    for d in range(n):
        for kind in (0, 1, 2):
            h_move(kind, d).wait_send()
        if d:
            give(d).wait_send()


def fast_body(
    queries_one, keys_one, values_one, queries_two, keys_two, values_two, key_offset,
    out_one, out_two, residual, norm_gain, routes, route_weight,
    expert_gate, expert_up, expert_down,
):
    n = lax.axis_size("sp")
    t = lax.axis_size("tp")
    rows, cols = residual.shape
    h1 = queries_one.shape[1] // DH1
    h2 = queries_two.shape[1] // DH2
    cap = 4 * rows // n
    vmem = pl.BlockSpec(memory_space=pltpu.VMEM)
    anyw = pl.BlockSpec(memory_space=pl.ANY)
    dma = pltpu.SemaphoreType.DMA
    large = (
        queries_one, keys_one, values_one, queries_two, keys_two, values_two,
        out_one, out_two, residual, expert_gate[0], expert_up[0], expert_down[0],
    )
    hid = expert_gate.shape[2]
    return pl.pallas_call(
        functools.partial(layer_kernel, n, t, h1, h2, cap),
        out_shape=pltpu.VMEM((rows, cols), BF),
        in_specs=[vmem] * 3 + [anyw] * 13,
        out_specs=vmem,
        scratch_shapes=[pltpu.VMEM(a.shape, a.dtype) for a in large[:6]]
        + [pltpu.VMEM((out_one.shape[0] + out_two.shape[0], out_one.shape[1]), BF)]
        + [pltpu.VMEM(a.shape, a.dtype) for a in large[8:]]
        + [
            pltpu.VMEM((1, cols), F32),
            pltpu.VMEM((h2, rows, DH1), BF),
            pltpu.VMEM((h2, rows // 2, DH1), BF),
            pltpu.VMEM((3, n, rows, DH1), BF),
            pltpu.VMEM((n, 8, rows), F32),
            pltpu.VMEM((n, 8, rows), F32),
            pltpu.VMEM((n, n, rows, DH1), F32),
            pltpu.VMEM((n, n, rows, DH1), F32),
            pltpu.VMEM((n, rows, DH1), BF),
            pltpu.VMEM((n, rows, DH1), BF),
            pltpu.VMEM((2, PIECES, rows, cols // PIECES), BF),
            pltpu.VMEM((2, PIECES, rows, cols // PIECES), BF),
            pltpu.VMEM((PIECES, rows, cols // PIECES), BF),
            pltpu.VMEM((PIECES, rows, cols // PIECES), BF),
            pltpu.VMEM((PIECES, rows, cols // PIECES), F32),
            pltpu.VMEM((1, 8, rows), F32),
            pltpu.VMEM((3, 8, rows), F32),
            pltpu.VMEM((n, 8, 128), F32),
            pltpu.VMEM((n, 8, 128), F32),
            pltpu.VMEM((rows, cols), BF),
            pltpu.VMEM((rows, cols), BF),
            pltpu.VMEM((2, rows, n * cap), BF),
            pltpu.VMEM((n * cap, rows), BF),
            pltpu.VMEM((2, rows, 128), F32),
            pltpu.VMEM((PARTS, n, cap, cols // PARTS), BF),
            pltpu.VMEM((t, PARTS, n, cap, cols // PARTS), BF),
            pltpu.VMEM((t, n, cap, hid), BF),
            pltpu.VMEM((n, cap, cols), BF),
            pltpu.VMEM((n, cap, cols), BF),
            dma((13,)),
            dma((n, 3)), dma((n, 3)),
            dma((n,)), dma((n,)),
            dma((n,)), dma((n,)),
            dma((2, PIECES)), dma((2, PIECES)),
            dma((PIECES,)), dma((PIECES,)),
            dma((3,)), dma((3,)),
            dma((n,)), dma((n,)),
            dma((n, PARTS)), dma((n, PARTS)),
            dma((3, n, PARTS)), dma((3, n, PARTS)),
            dma((3, n)), dma((3, n)),
            dma((n,)), dma((n,)),
        ],
        compiler_params=pltpu.CompilerParams(
            collective_id=0, has_side_effects=True, vmem_limit_bytes=60 * 2**20
        ),
        name="layer",
    )(
        key_offset.transpose(1, 2, 0), routes.T, route_weight.T, *large, norm_gain[None, :]
    )


def choose(*arrays):
    heads = arrays[0].shape[1] // DH1 + arrays[3].shape[1] // DH2
    n, t = lax.axis_size("sp"), lax.axis_size("tp")
    fits = heads == n and t == 4 and arrays[0].shape[0] == DH1 and DH1 == 2 * DH2
    fits = fits and arrays[0].shape[1] // DH1 * 2 == n and n == 8 and DH1 * 4 // n * 2 == 128
    return fast_body(*arrays) if fits else body(*arrays)


def solution(mesh):
    return jax.shard_map(
        choose,
        mesh=mesh,
        in_specs=(
            P("sp", "tp"),
            P("sp", "tp"),
            P("sp", "tp"),
            P("sp", "tp"),
            P("sp", "tp"),
            P("sp", "tp"),
            P("sp", None, "tp"),
            P("tp", None),
            P("tp", None),
            P("sp", "tp"),
            P(),
            P("sp", None),
            P("sp", None),
            P("sp", None, "tp"),
            P("sp", None, "tp"),
            P("sp", None, "tp"),
        ),
        out_specs=P("sp", "tp"),
        check_vma=False,
    )
```

```python
import functools

import jax
import jax.numpy as jnp
from jax import lax
from jax.experimental import pallas as pl
from jax.experimental.pallas import tpu as pltpu
from jax.sharding import PartitionSpec as P

DH1 = 128
DH2 = 64


EPS = 1e-06
PIECES = 4
PARTS = 2


def stick_group(query, keys, values, offset, head_size, own_start, key_block):
    row_count = query.shape[0]
    head_count = query.shape[1] // head_size
    query_heads = query.reshape(row_count, head_count, head_size)
    query_pos = own_start + jnp.arange(row_count, dtype=jnp.int32)
    block_count = (own_start + row_count + key_block - 1) // key_block

    def key_step(step_index, state_pair):
        summed, carried = state_pair
        first_key = (block_count - 1 - step_index) * key_block
        key_rows = lax.dynamic_slice_in_dim(keys, first_key, key_block, 0).reshape(
            key_block, head_count, head_size
        )
        value_rows = lax.dynamic_slice_in_dim(values, first_key, key_block, 0).reshape(
            key_block, head_count, head_size
        )
        bias_rows = lax.dynamic_slice_in_dim(offset, first_key, key_block, 0).astype(jnp.float32)
        scores = jnp.einsum(
            "qhd,khd->hqk", query_heads, key_rows, preferred_element_type=jnp.float32
        )
        scores = scores * head_size ** (-0.5) + bias_rows.T[:, None, :]
        key_pos = first_key + jnp.arange(key_block, dtype=jnp.int32)
        causal = key_pos[None, :] < query_pos[:, None]
        log_beta = jax.nn.log_sigmoid(scores)
        log_rest = jnp.where(causal, jax.nn.log_sigmoid(-scores), 0.0)
        shifted = jnp.pad(log_rest[..., 1:], ((0, 0), (0, 0), (0, 1)))
        within = lax.cumsum(shifted, axis=2, reverse=True)
        weights = jnp.where(causal, jnp.exp(log_beta + within + carried[..., None]), 0.0).astype(
            jnp.bfloat16
        )
        summed = summed + jnp.einsum(
            "hqk,khd->hqd", weights, value_rows, preferred_element_type=jnp.float32
        )
        carried = carried + jnp.sum(log_rest, axis=2)
        return (summed, carried)

    start_state = (
        jnp.zeros((head_count, row_count, head_size), jnp.float32),
        jnp.zeros((head_count, row_count), jnp.float32),
    )
    summed, _ = lax.fori_loop(0, block_count, key_step, start_state)
    return summed.transpose(1, 0, 2).reshape(row_count, head_count * head_size).astype(jnp.bfloat16)


def body(
    queries_one,
    keys_one,
    values_one,
    queries_two,
    keys_two,
    values_two,
    key_offset,
    out_one,
    out_two,
    residual,
    norm_gain,
    routes,
    route_weight,
    expert_gate,
    expert_up,
    expert_down,
):
    row_count = queries_one.shape[0]
    spread = lax.axis_size("sp")
    tp_count = lax.axis_size("tp")
    own_start = lax.axis_index("sp") * row_count
    factor = max(1, min(spread, 512 // row_count))
    while spread % factor:
        factor -= 1
    key_block = row_count * factor
    far_k1, far_v1, far_k2, far_v2, far_offset = (
        lax.all_gather(keys_one, "sp", axis=0, tiled=True),
        lax.all_gather(values_one, "sp", axis=0, tiled=True),
        lax.all_gather(keys_two, "sp", axis=0, tiled=True),
        lax.all_gather(values_two, "sp", axis=0, tiled=True),
        lax.all_gather(key_offset, "sp", axis=0, tiled=True),
    )
    attended_one = stick_group(
        queries_one, far_k1, far_v1, far_offset[:, 0, :], DH1, own_start, key_block
    )
    attended_two = stick_group(
        queries_two, far_k2, far_v2, far_offset[:, 1, :], DH2, own_start, key_block
    )
    partial_value = jnp.dot(attended_one, out_one, preferred_element_type=jnp.float32)
    partial_value = partial_value + jnp.dot(
        attended_two, out_two, preferred_element_type=jnp.float32
    )
    columns = residual.shape[1]
    column_start = lax.axis_index("tp") * columns
    resid_full = lax.all_gather(residual, "tp", axis=1, tiled=True)
    projected = lax.psum(partial_value.astype(jnp.bfloat16), "tp").astype(jnp.float32)
    stream = (resid_full.astype(jnp.float32) + projected).astype(jnp.bfloat16)
    stream_f = stream.astype(jnp.float32)
    normed = (
        stream_f * lax.rsqrt(jnp.mean(stream_f * stream_f, axis=1, keepdims=True) + EPS) * norm_gain
    ).astype(jnp.bfloat16)
    stream_own = lax.dynamic_slice_in_dim(stream, column_start, columns, 1)
    capacity = tp_count * ((4 * row_count // spread + tp_count - 1) // tp_count)
    flat_ids = routes.reshape(-1)
    onehot = (flat_ids[:, None] == jnp.arange(spread, dtype=jnp.int32)[None, :]).astype(jnp.int32)
    before = jnp.cumsum(onehot, axis=0) - onehot
    slot_of = flat_ids * capacity + jnp.sum(before * onehot, axis=1)
    chosen = slot_of[:, None] == jnp.arange(spread * capacity, dtype=jnp.int32)[None, :]
    selector = jnp.any(chosen.reshape(row_count, 2, spread * capacity), axis=1).T.astype(
        jnp.bfloat16
    )
    outgoing = jnp.dot(selector, normed, preferred_element_type=jnp.float32).astype(jnp.bfloat16)
    outgoing = outgoing.reshape(spread, capacity, normed.shape[1])
    gate_w = expert_gate[0]
    up_w = expert_up[0]
    down_w = expert_down[0]
    share_size = capacity // tp_count
    own_part = lax.dynamic_slice_in_dim(outgoing, lax.axis_index("tp") * share_size, share_size, 1)
    arrived = lax.all_to_all(own_part, "sp", split_axis=0, concat_axis=0, tiled=True)
    arrived = lax.all_gather(arrived, "tp", axis=1, tiled=True)
    sources, items, _ = arrived.shape
    flat_rows = arrived.reshape(sources * items, arrived.shape[2])
    gate_act = jnp.dot(flat_rows, gate_w, preferred_element_type=jnp.float32)
    up_act = jnp.dot(flat_rows, up_w, preferred_element_type=jnp.float32)
    hidden = (jax.nn.silu(gate_act) * up_act).astype(jnp.bfloat16)
    summed = jnp.dot(
        lax.all_gather(hidden, "tp", axis=1, tiled=True), down_w, preferred_element_type=jnp.float32
    )
    returned = lax.all_to_all(
        summed.astype(jnp.bfloat16).reshape(sources, items, down_w.shape[1]),
        "sp",
        split_axis=0,
        concat_axis=0,
        tiled=True,
    )
    back_rows = returned.reshape(spread * capacity, returned.shape[2])
    picked = jnp.dot(chosen.astype(jnp.bfloat16), back_rows, preferred_element_type=jnp.float32)
    picked = picked.reshape(row_count, 2, back_rows.shape[1])
    combined = route_weight[:, 0:1] * picked[:, 0] + route_weight[:, 1:2] * picked[:, 1]
    return (stream_own.astype(jnp.float32) + combined).astype(jnp.bfloat16)


BF = jnp.bfloat16
F32 = jnp.float32


def to(sp, tp):
    return {"device_id": (sp, tp), "device_id_type": pl.DeviceIdType.MESH}


def is_wide(index):
    return (index // 2 + index) % 2 == 0


def flipped(index, mask, n):
    place, total = 1, 0
    while place < n:
        bit = index // place % 2
        total = total + place * (1 - bit if mask & place else bit)
        place *= 2
    return total


def folded(block):
    half = block.shape[0] // 2
    return jnp.concatenate([block[:half, :DH2], block[half:, :DH2]], axis=1)


def unfolded(block):
    return jnp.concatenate([block[:, :DH2], block[:, DH2:]], axis=0)


SENDS = (
    ((1, 0), (4, 0)),
    ((4, 1), (1, 1), (2, 0), (2, 1), (5, 0)),
    ((5, 1), (3, 0), (3, 1), (6, 0), (6, 1), (7, 0), (7, 1)),
)
STEPS = (
    ("f", 1), ("f", 4), ("s"), ("f", 2), ("r", 0), ("r", 1), ("r", 4), ("f", 5), ("x", 4, 1),
    ("r", 2), ("f", 3), ("r", 5), ("x", 5, 2), ("f", 6), ("q", 4), ("q", 1), ("r", 3), ("h", 4, 1),
    ("f", 7), ("q", 5), ("q", 2), ("h", 5, 2), ("r", 6), ("x", 6, 3), ("r", 7), ("x", 7, 0), ("q", 6),
    ("q", 3), ("h", 6, 3), ("q", 7), ("q", 0), ("h", 7, 0),
)


def neighbours(tp, t):
    partner = tp + 1 - 2 * (tp % 2)
    across = (tp + 2) % t
    return partner, across, across + 1 - 2 * (across % 2)


def layer_kernel(
    n, t, h1, h2, cap,
    off_in, routes, route_weight,
    q1_hbm, k1_hbm, v1_hbm, q2_hbm, k2_hbm, v2_hbm, w1_hbm, w2_hbm, resid_hbm,
    gate_hbm, up_hbm, down_hbm, gain_hbm,
    out,
    q1_in, k1_in, v1_in, q2_in, k2_in, v2_in, w_in, resid_in, gate_in, up_in, down_in, gain,
    pk, pv, buf, off, offbuf, carry, acc, obuf, att,
    pair_out, pair_in, far_out, far_in, mine, stat_out, stat_in, fac_out, fac_in,
    stream_keep, scaled, chosen, picker, weights,
    sbuf, xbuf, hbuf, rbuf, backbuf,
    wsem, qs, qr, fs, fr, os_, or_, ps, pr, ys, yr, ss, sr, cs, cr,
    ds_, dr, xs, xr, hs, hr, rs, rr,
):
    in_hbm = (
        q1_hbm, k1_hbm, v1_hbm, q2_hbm, k2_hbm, v2_hbm, w1_hbm, w2_hbm, resid_hbm,
        gate_hbm, up_hbm, down_hbm,
    )
    in_vmem = (
        q1_in, k1_in, v1_in, q2_in, k2_in, v2_in,
        w_in.at[0 : h1 * DH1], w_in.at[h1 * DH1 :], resid_in, gate_in, up_in, down_in,
    )
    me = lax.axis_index("sp")
    tp = lax.axis_index("tp")
    partner, across, diagonal = neighbours(tp, t)
    rows, cols = resid_in.shape
    peers = [(lax.rem(me + d, n), tp) for d in range(1, n)]
    peers += [(me, peer) for peer in (partner, across, diagonal)]
    barrier = pltpu.get_barrier_semaphore()
    for peer in peers:
        pl.semaphore_signal(barrier, inc=1, **to(*peer))
    own_gain = gain_hbm.at[:, pl.ds(pl.multiple_of(tp * cols, 128), cols)]
    pairs = list(zip(in_hbm, in_vmem)) + [(own_gain, gain)]
    loads = [pltpu.make_async_copy(a, b, wsem.at[i]) for i, (a, b) in enumerate(pairs)]
    for load in loads:
        load.start()
    q1, k1, v1, q2, k2, v2 = in_vmem[:6]
    gate, up, down = in_vmem[9:]
    for load in loads[:6]:
        load.wait()
    for g in range(2):
        for h in range(off_in.shape[1]):
            off[2 * h + (h + g) % 2] = jnp.broadcast_to(off_in[g, h : h + 1, :].astype(F32), (8, rows))
    for h in range(h2):
        lanes = slice(h * DH2, (h + 1) * DH2)
        pk[h] = jnp.concatenate([q2[:, lanes], k2[:, lanes]], axis=1)
        pv[h] = folded(v2[:, lanes])
    pl.semaphore_wait(barrier, len(peers))

    def wide(dest, origin, d, part):
        src = (q1, k1, v1)[part]
        return pltpu.make_async_remote_copy(
            src.at[:, pl.ds(pl.multiple_of(dest // 2 * DH1, DH1), DH1)],
            buf.at[part, origin], qs.at[d, part], qr.at[d, part], **to(dest, tp),
        )

    def narrow(dest, origin, d, part):
        if part:
            src, dst = pv.at[dest // 2], buf.at[2, origin, 0 : rows // 2]
        else:
            src, dst = pk.at[dest // 2], buf.at[0, origin]
        return pltpu.make_async_remote_copy(src, dst, qs.at[d, part], qr.at[d, part], **to(dest, tp))

    def offs(dest, d):
        return pltpu.make_async_remote_copy(
            off.at[dest], offbuf.at[me], fs.at[d], fr.at[d], **to(dest, tp)
        )

    order = [d for pair in zip(range(n // 2, n), range(n // 2)) for d in pair if d]
    for d in order:
        dest = flipped(me, d, n)

        @pl.when(is_wide(dest))
        def _():
            for part in (0, 1, 2):
                wide(dest, me, d, part).start()

        @pl.when(jnp.logical_not(is_wide(dest)))
        def _():
            for part in (0, 2):
                narrow(dest, me, d, part).start()

        offs(dest, d).start()
    offbuf[me] = off[me]

    @pl.when(is_wide(me))
    def _():
        lanes = pl.ds(pl.multiple_of(me // 2 * DH1, DH1), DH1)
        buf[0, me] = q1[:, lanes]
        buf[1, me] = k1[:, lanes]
        buf[2, me] = v1[:, lanes]

    @pl.when(jnp.logical_not(is_wide(me)))
    def _():
        mine = me // 2
        buf[0, me] = pk[mine]
        buf[2, me, 0 : rows // 2] = pv[mine]

    table = jnp.concatenate(
        [routes[...].astype(F32), route_weight[...], jnp.zeros((128 - 4, rows), F32)], axis=0
    ).T
    lane = lax.broadcasted_iota(jnp.int32, (rows, 128), 1)
    row = lax.broadcasted_iota(jnp.int32, (rows, 128), 0)
    named = [table[:, k : k + 1] == lane.astype(F32) for k in (0, 1)]
    either = jnp.where(named[0] | named[1], 1.0, 0.0).astype(BF)
    earlier = jnp.where(lane < row, 1.0, 0.0).astype(BF)
    before = jnp.dot(earlier, either, preferred_element_type=F32)
    slots = lax.broadcasted_iota(jnp.int32, (rows, n * cap), 1).astype(F32)
    for k in (0, 1):
        slot = table[:, k : k + 1] * cap + jnp.sum(
            jnp.where(named[k], before, 0.0), axis=1, keepdims=True
        )
        chosen[k] = jnp.where(slots == slot, 1.0, 0.0).astype(BF)
        weights[k] = jnp.broadcast_to(table[:, 2 + k : 3 + k], (rows, 128))
    picker[...] = (chosen[0] + chosen[1]).astype(F32).T.astype(BF)

    lane = lax.broadcasted_iota(jnp.int32, (DH1, 2 * DH1), 1)
    row = lax.broadcasted_iota(jnp.int32, (DH1, 2 * DH1), 0)
    tri = jnp.where((row > lane) | (lane >= DH1), 1.0, 0.0).astype(BF)
    scale = jnp.where(is_wide(me), DH1 ** -0.5, DH2 ** -0.5).astype(F32)
    nt = (((1,), (1,)), ((), ()))

    def blocks(pairs):
        r = lax.broadcasted_iota(jnp.int32, (rows, rows), 0)
        c = lax.broadcasted_iota(jnp.int32, (rows, rows), 1)
        scores = [
            lax.dot_general(buf[0, i], buf[1, j], nt, preferred_element_type=F32)
            for i, j, _ in pairs
        ]
        betas, highs, lows = [], [], []
        for (_, j, own), s in zip(pairs, scores):
            s = s * scale + offbuf[j][0:1, :]
            soft = jnp.log(1.0 + jnp.exp(-jnp.abs(s)))
            log_beta = jnp.minimum(s, 0.0) - soft
            log_rest = log_beta - s
            if own:
                log_rest = jnp.where(c < r, log_rest, 0.0)
            high = log_rest.astype(BF)
            betas.append(log_beta)
            highs.append(high)
            lows.append((log_rest - high.astype(F32)).astype(BF))
        sums = [
            jnp.dot(high, tri, preferred_element_type=F32)
            + jnp.dot(low, tri, preferred_element_type=F32)
            for high, low in zip(highs, lows)
        ]
        weighted = []
        for (i, j, own), log_beta, total in zip(pairs, betas, sums):
            weight = jnp.exp(log_beta + total[:, :DH1])
            if own:
                weight = jnp.where(c < r, weight, 0.0)
            weighted.append(weight.astype(BF))
            carry[i, j] = total[:, DH1:]
        for (i, j, _), weight in zip(pairs, weighted):
            acc[i, j] = jnp.dot(weight, buf[2, j], preferred_element_type=F32)

    here = []
    for d in [0] + order:
        source = flipped(me, d, n)

        @pl.when(is_wide(me))
        def _():
            if d:
                for part in (0, 1, 2):
                    wide(source, me, d, part).wait_recv()

        @pl.when(jnp.logical_not(is_wide(me)))
        def _():
            if d:
                for part in (0, 2):
                    narrow(source, me, d, part).wait_recv()
            both = buf[0, source]
            zero = jnp.zeros((rows, DH1 - DH2), BF)
            buf[1, source] = jnp.concatenate([both[:, DH2:], zero], axis=1)
            buf[0, source] = jnp.concatenate([both[:, :DH2], zero], axis=1)
            buf[2, source] = jnp.concatenate(
                [unfolded(buf[2, source, 0 : rows // 2]), zero], axis=1
            )

        if d:
            offs(source, d).wait_recv()
        blocks(
            [(source, source, True)]
            + [(jnp.maximum(source, k), jnp.minimum(source, k), False) for k in here]
        )
        here.append(source)
    for i in range(n):
        total = acc[i, i]
        passed = carry[i, i]
        for j in range(i - 1, -1, -1):
            total = total + jnp.exp(passed) * acc[i, j]
            passed = passed + carry[i, j]
        obuf[i] = total.astype(BF)

    @pl.when(jnp.logical_not(is_wide(me)))
    def _():
        for i in range(n):
            obuf[i, 0 : rows // 2] = folded(obuf[i])

    def back(dest, d, full):
        part = slice(0, rows if full else rows // 2)
        return pltpu.make_async_remote_copy(
            obuf.at[dest, part], att.at[me, part], os_.at[d], or_.at[d], **to(dest, tp)
        )

    def each(test, act):
        for full in (True, False):

            @pl.when(test if full else jnp.logical_not(test))
            def _():
                act(full)

    each(
        is_wide(me),
        lambda full: [back(flipped(me, d, n), d, full).start() for d in order] and None,
    )
    att[me] = obuf[me]
    for d in order:
        dest = flipped(me, d, n)

        @pl.when(is_wide(dest))
        def _():
            for part in (0, 1, 2):
                wide(dest, me, d, part).wait_send()

        @pl.when(jnp.logical_not(is_wide(dest)))
        def _():
            for part in (0, 2):
                narrow(dest, me, d, part).wait_send()

        offs(dest, d).wait_send()
    for load in loads[6:9] + loads[12:]:
        load.wait()
    for d in order:
        dest = flipped(me, d, n)
        each(is_wide(dest), lambda full: back(dest, d, full).wait_recv())

    a1 = jnp.concatenate([att[2 * h + h % 2] for h in range(h1)], axis=1)
    a2 = jnp.concatenate(
        [unfolded(att[2 * h + 1 - h % 2, 0 : rows // 2]) for h in range(h2)], axis=1
    )

    a = jnp.concatenate([a1, a2], axis=1)
    pieces, _, width = mine.shape

    def partial(target, c):
        lanes = pl.ds(pl.multiple_of(target * cols + c * width, 128), width)
        return jnp.dot(a, w_in[:, lanes], preferred_element_type=F32)

    def pair(slot, c):
        return pltpu.make_async_remote_copy(
            pair_out.at[slot, c], pair_in.at[slot, c], ps.at[slot, c], pr.at[slot, c],
            **to(me, partner),
        )

    def far(c):
        return pltpu.make_async_remote_copy(
            far_out.at[c], far_in.at[c], ys.at[c], yr.at[c], **to(me, across)
        )

    for c in range(pieces):
        pair_out[0, c] = partial(diagonal, c).astype(BF)
        pair(0, c).start()
    for c in range(pieces):
        there = partial(across, c)
        pair(0, c).wait_recv()
        far_out[c] = (there + pair_in[0, c].astype(F32)).astype(BF)
        far(c).start()
    for c in range(pieces):
        pair_out[1, c] = partial(partner, c).astype(BF)
        pair(1, c).start()
    each(
        is_wide(me),
        lambda full: [back(flipped(me, d, n), d, full).wait_send() for d in order] and None,
    )
    for c in range(pieces):
        own = partial(tp, c)
        pair(1, c).wait_recv()
        mine[c] = own + pair_in[1, c].astype(F32)
    parts, _, _, wide_part = sbuf.shape
    per = pieces // parts

    def stat(slot, peer):
        return pltpu.make_async_remote_copy(
            stat_out.at[0], stat_in.at[slot], ss.at[slot], sr.at[slot], **to(me, peer)
        )

    def send(d, p):
        dest = flipped(me, d, n)
        return pltpu.make_async_remote_copy(
            sbuf.at[p, dest], xbuf.at[tp, p, me], ds_.at[d, p], dr.at[d, p], **to(dest, tp)
        )

    def x_move(kind, d, p):
        s = flipped(me, d, n)
        share = across if kind == 2 else tp
        peer = across if kind == 1 else partner
        return pltpu.make_async_remote_copy(
            xbuf.at[share, p, s], xbuf.at[share, p, s], xs.at[kind, d, p], xr.at[kind, d, p],
            **to(me, peer),
        )

    def h_move(kind, d):
        s = flipped(me, d, n)
        share = across if kind == 2 else tp
        peer = across if kind == 1 else partner
        return pltpu.make_async_remote_copy(
            hbuf.at[share, s], hbuf.at[share, s], hs.at[kind, d], hr.at[kind, d],
            **to(me, peer),
        )

    def factor(d):
        dest = flipped(me, d, n)
        return pltpu.make_async_remote_copy(
            fac_out.at[dest], fac_in.at[me], cs.at[d], cr.at[d], **to(dest, tp)
        )

    peers = tuple(enumerate((partner, across, diagonal)))
    squares = jnp.zeros((rows, 1), F32)
    for c in range(pieces):
        lanes = slice(c * width, (c + 1) * width)
        far(c).wait_recv()
        stream = (resid_in[:, lanes].astype(F32) + (mine[c] + far_in[c].astype(F32))).astype(BF)
        stream_keep[:, lanes] = stream
        stream = stream.astype(F32)
        scaled[:, lanes] = (stream * gain[:, lanes]).astype(BF)
        squares = squares + jnp.sum(stream * stream, axis=1, keepdims=True)
        if c == pieces - 1:
            stat_out[0] = jnp.broadcast_to(squares, (rows, 128)).T[0:8, :]
            for slot, peer in peers:
                stat(slot, peer).start()
        if (c + 1) % per == 0:
            p = c // per
            part = slice(p * wide_part, (p + 1) * wide_part)
            outgoing = jnp.dot(
                picker[...], scaled[:, part], preferred_element_type=F32
            ).astype(BF)
            for s in range(n):
                sbuf[p, s] = outgoing[s * cap : (s + 1) * cap]
            for d, q in SENDS[p]:
                send(d, q).start()
            xbuf[tp, p, me] = sbuf[p, me]
            x_move(1, 0, p).start()
            x_move(0, 0, p).start()
    def norms():
        for slot, peer in peers:
            stat(slot, peer).wait_recv()
        total = stat_out[0] + stat_in[0] + stat_in[1] + stat_in[2]
        total = jnp.broadcast_to(total[0:1, :], (128, rows)).T[:, 0:1]
        inverse = lax.rsqrt(total / (t * cols) + EPS)
        inverse = jnp.sum(
            (chosen[0] + chosen[1]).astype(F32) * inverse, axis=0, keepdims=True
        )
        for s in range(n):
            spot = inverse[:, s * cap : (s + 1) * cap]
            spot = jnp.concatenate([spot, jnp.zeros((1, 128 - cap), F32)], axis=1)
            fac_out[s] = jnp.broadcast_to(spot, (8, 128))
        for d in order:
            factor(d).start()
        fac_in[me] = fac_out[me]
        for d, q in SENDS[-1]:
            send(d, q).start()

    def give(d):
        dest = flipped(me, d, n)
        return pltpu.make_async_remote_copy(
            rbuf.at[dest], backbuf.at[me], rs.at[d], rr.at[d], **to(dest, tp)
        )

    for load in loads[9:12]:
        load.wait()

    def relay(move):
        move(1).wait_recv()
        move(2).start()

    def settle(move):
        move(0).wait_recv()
        move(2).wait_recv()

    def enter(members):
        for d in members:
            if d:
                factor(d).wait_recv()
            for p in range(parts):
                settle(lambda kind: x_move(kind, d, p))
        sources = [flipped(me, d, n) for d in members]
        column = jnp.concatenate([fac_in[s][0:1, :cap] for s in sources], axis=1)
        column = jnp.broadcast_to(column, (128, len(members) * cap)).T[:, 0:1]
        gated = jnp.zeros((len(members) * cap, gate.shape[1]), F32)
        upped = gated
        for j in range(t):
            for p in range(parts):
                x = jnp.concatenate([xbuf[j, p, s] for s in sources], axis=0)
                first = j * cols + p * wide_part
                gated = gated + jnp.dot(
                    x, gate[first : first + wide_part, :], preferred_element_type=F32
                )
                upped = upped + jnp.dot(
                    x, up[first : first + wide_part, :], preferred_element_type=F32
                )
        gated = gated * column
        hidden = (gated / (1.0 + jnp.exp(-gated)) * (upped * column)).astype(BF)
        for k, d in enumerate(members):
            hbuf[tp, sources[k]] = hidden[k * cap : (k + 1) * cap]
            h_move(1, d).start()
            h_move(0, d).start()

    def leave(members):
        for d in members:
            settle(lambda kind: h_move(kind, d))
        sources = [flipped(me, d, n) for d in members]
        size = hbuf.shape[3]
        done = jnp.zeros((len(members) * cap, down.shape[1]), F32)
        for j in range(t):
            h = jnp.concatenate([hbuf[j, s] for s in sources], axis=0)
            done = done + jnp.dot(
                h, down[j * size : (j + 1) * size, :], preferred_element_type=F32
            )
        done = done.astype(BF)
        for k, d in enumerate(members):
            rbuf[sources[k]] = done[k * cap : (k + 1) * cap]
            if d:
                give(d).start()

    for kind, *members in STEPS:
        if kind == "s":
            norms()
        elif kind == "f":
            for p in range(parts):
                send(members[0], p).wait_recv()
                x_move(1, members[0], p).start()
                x_move(0, members[0], p).start()
        elif kind == "r":
            for p in range(parts):
                relay(lambda k: x_move(k, members[0], p))
        elif kind == "x":
            enter(members)
        elif kind == "q":
            relay(lambda k: h_move(k, members[0]))
        else:
            if (kind, *members) == STEPS[-1]:
                for d in range(n):
                    for p in range(parts):
                        for k in (0, 1, 2):
                            x_move(k, d, p).wait_send()
                        if d:
                            send(d, p).wait_send()
                    if d:
                        factor(d).wait_send()
                for c in range(pieces):
                    pair(0, c).wait_send()
                    pair(1, c).wait_send()
                    far(c).wait_send()
                for slot, peer in peers:
                    stat(slot, peer).wait_send()
            leave(members)
    backbuf[me] = rbuf[me]
    total = stream_keep[...].astype(F32)
    for first in (4, 2, 0, 6):
        for d in (first, first + 1):
            if d:
                give(d).wait_recv()
        base = flipped(me, first, n) // 2
        lanes = pl.ds(pl.multiple_of(base * 2 * cap, 2 * cap), 2 * cap)
        both = jnp.concatenate([backbuf[2 * base], backbuf[2 * base + 1]], axis=0)
        for k in (0, 1):
            total = total + weights[k][:, 0:1] * jnp.dot(
                chosen[k, :, lanes], both, preferred_element_type=F32
            )
    out[...] = total.astype(BF)
    for d in range(n):
        for kind in (0, 1, 2):
            h_move(kind, d).wait_send()
        if d:
            give(d).wait_send()


def fast_body(
    queries_one, keys_one, values_one, queries_two, keys_two, values_two, key_offset,
    out_one, out_two, residual, norm_gain, routes, route_weight,
    expert_gate, expert_up, expert_down,
):
    n = lax.axis_size("sp")
    t = lax.axis_size("tp")
    rows, cols = residual.shape
    h1 = queries_one.shape[1] // DH1
    h2 = queries_two.shape[1] // DH2
    cap = 4 * rows // n
    vmem = pl.BlockSpec(memory_space=pltpu.VMEM)
    anyw = pl.BlockSpec(memory_space=pl.ANY)
    dma = pltpu.SemaphoreType.DMA
    large = (
        queries_one, keys_one, values_one, queries_two, keys_two, values_two,
        out_one, out_two, residual, expert_gate[0], expert_up[0], expert_down[0],
    )
    hid = expert_gate.shape[2]
    return pl.pallas_call(
        functools.partial(layer_kernel, n, t, h1, h2, cap),
        out_shape=pltpu.VMEM((rows, cols), BF),
        in_specs=[vmem] * 3 + [anyw] * 13,
        out_specs=vmem,
        scratch_shapes=[pltpu.VMEM(a.shape, a.dtype) for a in large[:6]]
        + [pltpu.VMEM((out_one.shape[0] + out_two.shape[0], out_one.shape[1]), BF)]
        + [pltpu.VMEM(a.shape, a.dtype) for a in large[8:]]
        + [
            pltpu.VMEM((1, cols), F32),
            pltpu.VMEM((h2, rows, DH1), BF),
            pltpu.VMEM((h2, rows // 2, DH1), BF),
            pltpu.VMEM((3, n, rows, DH1), BF),
            pltpu.VMEM((n, 8, rows), F32),
            pltpu.VMEM((n, 8, rows), F32),
            pltpu.VMEM((n, n, rows, DH1), F32),
            pltpu.VMEM((n, n, rows, DH1), F32),
            pltpu.VMEM((n, rows, DH1), BF),
            pltpu.VMEM((n, rows, DH1), BF),
            pltpu.VMEM((2, PIECES, rows, cols // PIECES), BF),
            pltpu.VMEM((2, PIECES, rows, cols // PIECES), BF),
            pltpu.VMEM((PIECES, rows, cols // PIECES), BF),
            pltpu.VMEM((PIECES, rows, cols // PIECES), BF),
            pltpu.VMEM((PIECES, rows, cols // PIECES), F32),
            pltpu.VMEM((1, 8, rows), F32),
            pltpu.VMEM((3, 8, rows), F32),
            pltpu.VMEM((n, 8, 128), F32),
            pltpu.VMEM((n, 8, 128), F32),
            pltpu.VMEM((rows, cols), BF),
            pltpu.VMEM((rows, cols), BF),
            pltpu.VMEM((2, rows, n * cap), BF),
            pltpu.VMEM((n * cap, rows), BF),
            pltpu.VMEM((2, rows, 128), F32),
            pltpu.VMEM((PARTS, n, cap, cols // PARTS), BF),
            pltpu.VMEM((t, PARTS, n, cap, cols // PARTS), BF),
            pltpu.VMEM((t, n, cap, hid), BF),
            pltpu.VMEM((n, cap, cols), BF),
            pltpu.VMEM((n, cap, cols), BF),
            dma((13,)),
            dma((n, 3)), dma((n, 3)),
            dma((n,)), dma((n,)),
            dma((n,)), dma((n,)),
            dma((2, PIECES)), dma((2, PIECES)),
            dma((PIECES,)), dma((PIECES,)),
            dma((3,)), dma((3,)),
            dma((n,)), dma((n,)),
            dma((n, PARTS)), dma((n, PARTS)),
            dma((3, n, PARTS)), dma((3, n, PARTS)),
            dma((3, n)), dma((3, n)),
            dma((n,)), dma((n,)),
        ],
        compiler_params=pltpu.CompilerParams(
            collective_id=0, has_side_effects=True, vmem_limit_bytes=60 * 2**20
        ),
        name="layer",
    )(
        key_offset.transpose(1, 2, 0), routes.T, route_weight.T, *large, norm_gain[None, :]
    )


def choose(*arrays):
    heads = arrays[0].shape[1] // DH1 + arrays[3].shape[1] // DH2
    n, t = lax.axis_size("sp"), lax.axis_size("tp")
    fits = heads == n and t == 4 and arrays[0].shape[0] == DH1 and DH1 == 2 * DH2
    fits = fits and arrays[0].shape[1] // DH1 * 2 == n and n == 8 and DH1 * 4 // n * 2 == 128
    return fast_body(*arrays) if fits else body(*arrays)


def solution(mesh):
    return jax.shard_map(
        choose,
        mesh=mesh,
        in_specs=(
            P("sp", "tp"),
            P("sp", "tp"),
            P("sp", "tp"),
            P("sp", "tp"),
            P("sp", "tp"),
            P("sp", "tp"),
            P("sp", None, "tp"),
            P("tp", None),
            P("tp", None),
            P("sp", "tp"),
            P(),
            P("sp", None),
            P("sp", None),
            P("sp", None, "tp"),
            P("sp", None, "tp"),
            P("sp", None, "tp"),
        ),
        out_specs=P("sp", "tp"),
        check_vma=False,
    )
```
